32 devices in a mesh: ep: 8 (over z, y), tp: 4 (over x, core).
Axes of the slice: x: 2, y: 2, z: 4, core: 2. Of those that a mesh axis runs over, the one named last changes fastest.
Arguments:
- hidden: bfloat16 [512, 2048], P('ep'), may hold values from -10 to 10
- mix_gain: bfloat16 [2048], replicated, may hold values from 0.099609375 to 1.8984375
- proj_x: bfloat16 [2048, 2048], P('ep', 'tp'), may hold values from -0.125 to 0.125
- proj_y: bfloat16 [2048, 2048], P('ep', 'tp'), may hold values from -0.125 to 0.125
- conv_taps: bfloat16 [4, 2048], P(None, 'tp'), may hold values from -3 to 3
- input_gate: bfloat16 [32, 64, 64], P('tp'), may hold values from -0.75 to 0.75
- decay_gate: bfloat16 [32, 64, 64], P('tp'), may hold values from -0.75 to 0.75
- decay_param: float32 [2048], P('tp'), may hold values from 1 to 6
- proj_out: bfloat16 [2048, 2048], P('tp'), may hold values from -0.125 to 0.125
- conv_state: bfloat16 [512, 3, 2048], P('ep', None, 'tp'), may hold values from -6 to 6
- lru_state: float32 [512, 2048], P('ep', 'tp'), may hold values from -6 to 6
- ffn_gain: bfloat16 [2048], replicated, may hold values from 0.099609375 to 1.8984375
- routes: int32 [512, 2], P('ep'), may hold values from 0 to 7, all different within a row; in each aligned block of 64 rows (0 to 63, 64 to 127, ...) at most 18 rows name the same one
- route_weights: float32 [512, 2], P('ep'), may hold values from 0.2 to 1
- expert_gate: bfloat16 [8, 2048, 3072], P('ep', None, 'tp'), may hold values from -0.125 to 0.125
- expert_up: bfloat16 [8, 2048, 3072], P('ep', None, 'tp'), may hold values from -0.125 to 0.125
- expert_down: bfloat16 [8, 3072, 2048], P('ep', 'tp'), may hold values from -0.109375 to 0.109375
- dense_gate: bfloat16 [2048, 6144], P('tp', 'ep'), may hold values from -0.125 to 0.125
- dense_up: bfloat16 [2048, 6144], P('tp', 'ep'), may hold values from -0.125 to 0.125
- dense_down: bfloat16 [6144, 2048], P('ep', 'tp'), may hold values from -0.078125 to 0.078125
- branch_gate: float32 [2048], P('tp'), may hold values from -4 to 4
Outputs:
- new_hidden: bfloat16 [512, 2048], P('ep', 'tp')
- new_lru: float32 [512, 2048], P('ep', 'tp')
- new_conv: bfloat16 [512, 3, 2048], P('ep', None, 'tp')
The draws below stay inside these ranges and needn't reach their ends.
Inputs may be any that keep to these rules, and one draw needn't show every extreme that they name: `routes`: each row names 2 different experts. In the 64 rows of one index of ep, no expert is named by more than 18 rows, a bound that some block reaches.
All inputs are finite; a program needn't handle non-finite values.
Results may differ from the reference program's by a relative error of at most 0.017.
Values may be sent and summed in bfloat16 or wider, within the bound.
A program may use at most 128 MiB of HBM per device.

```python
import math
import jax
import jax.numpy as jnp
import numpy as np
from jax import lax

D = 2048
HEADS = 32
BLOCK = 64
LRU = 2048
TAPS = 4
FFE = 3072
DFF = 6144
EXPERTS = 8
TOPK = 2
SEQ_DEV = 64
BATCH = 512
CAP = 18
N_EP = 8
N_TP = 4


def draw_hidden(key, part):
    noise_key = jax.random.fold_in(key, 11)
    column = jnp.arange(D, dtype=jnp.float32) / (D - 1)
    scales = 0.5 * jnp.power(4.0, column)
    values = jax.random.normal(noise_key, (BATCH, D), jnp.float32) * scales[None, :]
    return jnp.clip(values, -10.0, 10.0).astype(jnp.bfloat16)


def shard_levels(rng, shape, cuts, smallest, top_value):
    loudness = 1.0
    for dim, shards_of in cuts:
        draws = jax.random.uniform(jax.random.fold_in(jax.random.fold_in(rng, 6), dim), (shards_of,), jnp.float32, smallest / len(cuts), top_value / len(cuts))
        loudness = loudness * jnp.repeat(jnp.exp(draws), shape[dim] // shards_of).reshape((-1,) + (1,) * (len(shape) - 1 - dim))
    return loudness


def assign_block(key, own, number, rows, count, top, reach, slope):
    sequence = jax.random.permutation(key, count)
    crowded, common = portions_of(count, rows * top, reach, slope, True), portions_of(count, rows * top, reach, slope, False)
    places = jnp.arange(count)

    def named(lengths, turn):
        used = int((lengths > 0).sum())
        fixed = max(1, used // 4)
        passed = fixed + (places - fixed + turn * (used - fixed)) % max(1, count - fixed)
        return jnp.zeros((count,), jnp.int32).at[sequence[jnp.where(places < fixed, places, passed)]].set(jnp.asarray(lengths, jnp.int32))

    lengths = jnp.where(number % 4 == 0, named(crowded, number // 4), named(common, number - number // 4 - 1))
    mixed = jax.random.permutation(jax.random.fold_in(own, 3), count)
    source_of, receiver = mixed[0:count // 2 * 2:2], mixed[1:count // 2 * 2:2]
    margin = jnp.minimum(lengths[source_of] - 1, reach - lengths[receiver]) // 2
    margin = jnp.where((source_of == sequence[0]) | (receiver == sequence[0]) | (lengths[receiver] == 0), 0, jnp.maximum(margin, 0))
    passed = jax.random.randint(jax.random.fold_in(own, 4), (count // 2,), 0, 1 << 20) % (margin + 1)
    lengths = lengths.at[source_of].add(-passed).at[receiver].add(passed)
    labels = jnp.searchsorted(jnp.cumsum(lengths), jnp.arange(rows * top), side="right").astype(jnp.int32)
    listing = labels.reshape(top, rows).T
    listing = listing[jax.random.permutation(jax.random.fold_in(own, 1), rows)]
    turn = jax.random.randint(jax.random.fold_in(own, 2), (rows, 1), 0, top)
    return jnp.take_along_axis(listing, (jnp.arange(top)[None, :] + turn) % top, axis=1)


def portions_of(count, total, limit, lean, full):
    portions = [(1 << 20) // math.isqrt(rank ** lean) + 1 for rank in range(1, count + 1)]
    largest = limit if full else min(limit, max(-(-total // count), total * portions[0] // sum(portions)))
    least = 1 if total - largest >= count - 1 else 0
    counts, rest = [largest] + [least] * (count - 1), total - largest - least * (count - 1)
    while rest > 0:
        movable = [i for i in range(1, count) if counts[i] < largest] or [i for i in range(1, count) if counts[i] < limit]
        whole, budget = sum([portions[i] for i in movable]), rest
        for i in movable:
            addition = min(limit - counts[i], max(1, budget * portions[i] // whole), rest)
            counts[i] = counts[i] + addition
            rest = rest - addition
    return np.array(counts)


def bell_draw(stream_key, dims, spread, reach, split=(), held_as=jnp.bfloat16):
    values = jax.random.normal(stream_key, dims, jnp.float32) * spread
    if len(split) > 0:
        values = shard_levels(stream_key, dims, split, -0.22, 0.18) * values
    return jnp.clip(values, min=-reach, max=reach).astype(held_as)


def setup_inputs(seed: int = 0) -> dict:
    streams_of = jax.random.split(jax.random.key(seed), 22)
    hidden = draw_hidden(jax.random.fold_in(streams_of[21], 71), 0)
    mix_gain = jnp.clip(1.0 + 0.18 * jax.random.normal(streams_of[1], (D,), jnp.float32), 0.099609375, 1.8984375).astype(jnp.bfloat16)
    proj_x = bell_draw(streams_of[2], (D, LRU), D ** -0.5, 0.125, ((0, 8), (1, 4)))
    proj_y = bell_draw(streams_of[3], (D, LRU), D ** -0.5, 0.125, ((0, 8), (1, 4)))
    conv_taps = bell_draw(streams_of[4], (TAPS, LRU), 0.5, 3.0, ((1, 4),))
    input_gate = bell_draw(streams_of[5], (HEADS, BLOCK, BLOCK), BLOCK ** -0.5, 0.75, ((0, 4),))
    decay_gate = bell_draw(streams_of[6], (HEADS, BLOCK, BLOCK), BLOCK ** -0.5, 0.75, ((0, 4),))
    decay_param = jnp.clip(1.0 + 5.0 * jax.random.uniform(streams_of[7], (LRU,), jnp.float32) ** shard_levels(streams_of[7], (LRU,), ((0, 4),), -0.2, 0.2), 1.0, 6.0)
    proj_out = bell_draw(streams_of[8], (LRU, D), LRU ** -0.5, 0.125, ((0, 4),))
    conv_state = bell_draw(streams_of[9], (BATCH, TAPS - 1, LRU), 1.0, 6.0, ((0, 8), (2, 4)))
    lru_state = bell_draw(streams_of[10], (BATCH, LRU), 1.0, 6.0, ((0, 8), (1, 4)), jnp.float32)
    ffn_gain = jnp.clip(1.0 + 0.18 * jax.random.normal(streams_of[11], (D,), jnp.float32), 0.099609375, 1.8984375).astype(jnp.bfloat16)
    routes_keys = jax.random.split(jax.random.fold_in(streams_of[12], 1), BATCH // SEQ_DEV)
    routes_turns = jax.random.permutation(jax.random.fold_in(streams_of[12], 3), BATCH // SEQ_DEV)
    routes = jax.vmap(lambda own, number: assign_block(jax.random.fold_in(streams_of[12], 2), own, number, SEQ_DEV, EXPERTS, TOPK, CAP, 1))(routes_keys, routes_turns).reshape((BATCH, TOPK))
    route_weights = jnp.clip(jnp.exp(math.log(1.0) - 1.609438 * jax.random.uniform(streams_of[13], (BATCH, TOPK), jnp.float32) ** shard_levels(streams_of[13], (BATCH, TOPK), ((0, 8),), -0.2, 0.2)), 0.2, 1.0)
    expert_gate = bell_draw(streams_of[14], (EXPERTS, D, FFE), D ** -0.5, 0.125, ((0, 8), (2, 4)))
    expert_up = bell_draw(streams_of[15], (EXPERTS, D, FFE), D ** -0.5, 0.125, ((0, 8), (2, 4)))
    expert_down = bell_draw(streams_of[16], (EXPERTS, FFE, D), FFE ** -0.5, 0.109375, ((0, 8), (1, 4)))
    dense_gate = bell_draw(streams_of[17], (D, DFF), D ** -0.5, 0.125, ((0, 4), (1, 8)))
    dense_up = bell_draw(streams_of[18], (D, DFF), D ** -0.5, 0.125, ((0, 4), (1, 8)))
    dense_down = bell_draw(streams_of[19], (DFF, D), DFF ** -0.5, 0.078125, ((0, 8), (1, 4)))
    branch_gate = bell_draw(streams_of[20], (D,), 1.0, 4.0, ((0, 4),), jnp.float32)
    return dict(hidden=hidden, mix_gain=mix_gain, proj_x=proj_x, proj_y=proj_y, conv_taps=conv_taps, input_gate=input_gate, decay_gate=decay_gate, decay_param=decay_param, proj_out=proj_out, conv_state=conv_state, lru_state=lru_state, ffn_gain=ffn_gain, routes=routes, route_weights=route_weights, expert_gate=expert_gate, expert_up=expert_up, expert_down=expert_down, dense_gate=dense_gate, dense_up=dense_up, dense_down=dense_down, branch_gate=branch_gate)


epsilon = 1e-06
decay_scale = 8.0

def rms_scale(values, gain_vec):
    floats = values.astype(jnp.float32)
    meansq = lax.optimization_barrier(jnp.mean(floats * floats, axis=-1, keepdims=True))
    return floats * lax.rsqrt(meansq + epsilon) * gain_vec.astype(jnp.float32)

def reference(hidden, mix_gain, proj_x, proj_y, conv_taps, input_gate, decay_gate, decay_param, proj_out, conv_state, lru_state, ffn_gain, routes, route_weights, expert_gate, expert_up, expert_down, dense_gate, dense_up, dense_down, branch_gate):
    batch_rows = hidden.shape[0]
    lru_width = HEADS * BLOCK
    normed = rms_scale(hidden, mix_gain).astype(jnp.bfloat16)
    x_proj = jnp.dot(normed, proj_x, preferred_element_type=jnp.float32).astype(jnp.bfloat16)
    y_proj = jnp.dot(normed, proj_y, preferred_element_type=jnp.float32).astype(jnp.bfloat16)
    window = jnp.concatenate([conv_state, x_proj[:, None, :]], axis=1)
    conv_out = lax.optimization_barrier(jnp.sum(window.astype(jnp.float32) * conv_taps.astype(jnp.float32)[None], axis=1)).astype(jnp.bfloat16)
    heads_in = conv_out.astype(jnp.float32).reshape(batch_rows, HEADS, BLOCK)
    gate_in = jax.nn.sigmoid(jnp.einsum('bhi,hij->bhj', heads_in, input_gate.astype(jnp.float32)).reshape(batch_rows, lru_width))
    gate_dec = jax.nn.sigmoid(jnp.einsum('bhi,hij->bhj', heads_in, decay_gate.astype(jnp.float32)).reshape(batch_rows, lru_width))
    log_decay = decay_scale * gate_dec * jax.nn.log_sigmoid(decay_param)
    decay_rate = jnp.exp(log_decay)
    inject = jnp.sqrt(-jnp.expm1(2.0 * log_decay))
    new_lru = decay_rate * lru_state + inject * gate_in * conv_out.astype(jnp.float32)
    gated_out = (new_lru * jax.nn.gelu(y_proj.astype(jnp.float32))).astype(jnp.bfloat16)
    head_share = lru_width // N_TP
    mixer_sum = jnp.zeros((batch_rows, D), jnp.float32)
    for member in range(N_TP):
        partial_value = jnp.dot(gated_out[:, member * head_share:(member + 1) * head_share], proj_out[member * head_share:(member + 1) * head_share], preferred_element_type=jnp.float32).astype(jnp.bfloat16)
        mixer_sum = mixer_sum + partial_value.astype(jnp.float32)
    summed = (hidden.astype(jnp.float32) + mixer_sum).astype(jnp.bfloat16)
    ffn_in = rms_scale(summed, ffn_gain).astype(jnp.bfloat16)
    pair_expert = routes.reshape(-1).astype(jnp.int32)
    onehot = (pair_expert[:, None] == jnp.arange(EXPERTS, dtype=jnp.int32)[None, :]).astype(jnp.int32)
    grouped = onehot.reshape(N_EP, SEQ_DEV * TOPK, EXPERTS)
    before = jnp.cumsum(grouped, axis=1) - grouped
    slot_rank = lax.optimization_barrier(jnp.sum(before * grouped, axis=2)).reshape(-1)
    group_of = jnp.arange(BATCH * TOPK, dtype=jnp.int32) // (SEQ_DEV * TOPK)
    position = (group_of * CAP + slot_rank).astype(jnp.int32)
    token_of = jnp.arange(BATCH * TOPK, dtype=jnp.int32) // TOPK
    buffer = jnp.zeros((EXPERTS, N_EP * CAP, D), jnp.bfloat16).at[pair_expert, position].set(ffn_in[token_of])
    ff_share = FFE // N_TP

    def one_expert(operands):
        slot_rows, gate_w, up_w, down_w = operands
        gate_val = jnp.dot(slot_rows, gate_w, preferred_element_type=jnp.float32)
        up_val = jnp.dot(slot_rows, up_w, preferred_element_type=jnp.float32)
        inner_act = (jax.nn.silu(gate_val) * up_val).astype(jnp.bfloat16)
        total_out = jnp.zeros((slot_rows.shape[0], D), jnp.float32)
        for member in range(N_TP):
            piece_out = jnp.dot(inner_act[:, member * ff_share:(member + 1) * ff_share], down_w[member * ff_share:(member + 1) * ff_share], preferred_element_type=jnp.float32).astype(jnp.bfloat16)
            total_out = total_out + piece_out.astype(jnp.float32)
        return total_out.astype(jnp.bfloat16)
    results = lax.map(one_expert, (buffer, expert_gate, expert_up, expert_down))
    picked = results[pair_expert, position].astype(jnp.float32)
    expert_sum = lax.optimization_barrier(jnp.sum((picked * route_weights.reshape(-1)[:, None]).reshape(batch_rows, TOPK, D), axis=1))
    dense_g = jnp.dot(ffn_in, dense_gate, preferred_element_type=jnp.float32)
    dense_u = jnp.dot(ffn_in, dense_up, preferred_element_type=jnp.float32)
    dense_hid = (jax.nn.silu(dense_g) * dense_u).astype(jnp.bfloat16)
    dense_out = jnp.dot(dense_hid, dense_down, preferred_element_type=jnp.float32)
    new_hidden = (summed.astype(jnp.float32) + expert_sum + jax.nn.sigmoid(branch_gate)[None, :] * dense_out).astype(jnp.bfloat16)
    return (new_hidden, new_lru, window[:, 1:])
```

```python
import functools

import jax
import jax.numpy as jnp
from jax import lax
from jax.experimental import pallas as pl
from jax.experimental.pallas import tpu as pltpu
from jax.sharding import PartitionSpec as P

epsilon = 1e-06
decay_scale = 8.0
MESH = pl.DeviceIdType.MESH
F32 = jnp.float32
BF16 = jnp.bfloat16


def dot(a, b):
    return jnp.dot(a, b, preferred_element_type=F32)


def layer_kernel(
    E, T, cap,
    hidden, mix_gain, routes, weights, conv_old, taps, ig, dgate, decay_param, lru, ffn_gain, branch,
    wx_h, wy_h, dg_h, du_h, po_h, eg_h, eu_h, ed_h, dd_h,
    new_hidden, new_lru, conv_new,
    ct, w_ref, bd, wx, wy, dg, du, po, eg, eu, ed, dd, nb, dwp, dwr, spread, pm, pacc, yrec, zout, zrec, ctr, acc,
    mbuf, mrec, srow, prow, xall, aall, xe, hid, sel, own_sel, w_slot, s_slot,
    ebuf, erec, epart, ex, exr, eo, eor, dtmp, om, dacc, orm, oz, ozr, summed_ref,
    load_sem, nb_s, nb_r, ct_s, ct_r, pm_s, pm_r, pz_s, pz_r, dw_s, dw_r, mx_s, mx_r, q_s, q_r,
    xr_s, xf_s, xs_s, xd_s, x_r, a_s, a_r, ed_s, ed_r, ex_s, ex_r, eo_s, eo_r, om_s, om_r, oz_s, oz_r,
):
    e = lax.axis_index("ep")
    t = lax.axis_index("tp")
    M, D = hidden.shape
    C = D // T
    R = wx.shape[0]
    G = E // 2
    g0 = e // 2
    par = lax.rem(e, 2)
    mate = e + 1 - 2 * par
    own_cols = pl.ds(pl.multiple_of(t * C, 128), C)

    def ep_peer(k):
        return lax.rem(e + k, E)

    def ep_from(k):
        return lax.rem(e + E - k, E)

    def group(k):
        return lax.rem(g0 + k, G)

    def rail_from(k):
        return 2 * lax.rem(g0 + G - k, G) + par

    def mate_of(s):
        return s + 1 - 2 * lax.rem(s, 2)

    def peer_group(k):
        if G & (G - 1):
            return lax.rem(g0 + k, G)
        g, bit = 0, 1
        while bit < G:
            g = g + bit * lax.rem(g0 // bit + k // bit, 2)
            bit *= 2
        return g

    def tp_peer(k):
        return lax.rem(t + k, T)

    across = lax.rem(t + T // 2, T)
    beside = t + 1 - 2 * lax.rem(t, 2)
    diagonal = lax.rem(beside + T // 2, T)

    loads = [
        pltpu.make_async_copy(src, dst, load_sem.at[i])
        for i, (src, dst) in enumerate(
            ((po_h, po), (eg_h, eg), (eu_h, eu), (ed_h, ed), (dd_h, dd),
             (wx_h, wx), (wy_h, wy), (dg_h, dg), (du_h, du))
        )
    ]
    own_dw = pltpu.make_async_copy(dwp.at[t], dwr.at[t], load_sem.at[9])
    for i in (5, 6, 7, 8, 0):
        loads[i].start()

    def rcopy(src, dst, s, r, ep=None, tp=None):
        return pltpu.make_async_remote_copy(
            src_ref=src, dst_ref=dst, send_sem=s, recv_sem=r,
            device_id=(e if ep is None else ep, t if tp is None else tp),
            device_id_type=MESH,
        )

    barrier = pltpu.get_barrier_semaphore()

    @pl.loop(1, E)
    def _(k):
        pl.semaphore_signal(barrier, inc=1, device_id=(ep_peer(k), t), device_id_type=MESH)

    for k in range(1, T):
        pl.semaphore_signal(barrier, inc=1, device_id=(e, tp_peer(k)), device_id_type=MESH)
    hf = hidden[...].astype(F32)
    inv = lax.rsqrt(jnp.mean(hf * hf, axis=-1, keepdims=True) + epsilon)
    normed = (hf * inv * mix_gain[...].reshape(1, D).astype(F32)).astype(BF16)
    for p in range(E):
        nb[p] = normed[:, p * R:(p + 1) * R]
    for p in range(E):
        ct[p] = jnp.sum(jnp.where(routes[...] == p, weights[...], 0.0), axis=0, keepdims=True)
    pl.semaphore_wait(barrier, E - 1 + T - 1)

    @pl.loop(1, E)
    def _(k):
        p = ep_peer(k)
        rcopy(nb.at[p], spread.at[e], nb_s.at[p], nb_r.at[e], ep=p).start()
        rcopy(ct.at[p], ctr.at[e], ct_s.at[p], ct_r.at[e], ep=p).start()

    loads[7].wait()
    loads[8].wait()
    h = dg.shape[1] // T
    half = dwp.shape[2] // 2
    if half != h:
        dwp[...] = jnp.zeros_like(dwp)
    for j in range(T):
        dwp[j, :, :h] = dg[:, j * h:(j + 1) * h]
        dwp[j, :, half:half + h] = du[:, j * h:(j + 1) * h]
    own_dw.start()
    for k in range(1, T):
        j = tp_peer(k)
        rcopy(dwp.at[j], dwr.at[t], dw_s.at[j], dw_r.at[t], tp=j).start()
    for l in loads[1:5]:
        l.start()

    spread[e] = nb[e]
    loads[5].wait()
    loads[6].wait()

    def arrive(s):
        rcopy(nb.at[s], spread.at[s], nb_s.at[s], nb_r.at[s], ep=s).wait_recv()

    def share(g):
        blk = spread[2 * g + 1 - par]
        pm[g, :, :C] = dot(blk, wx[...]).astype(BF16)
        pm[g, :, C:] = dot(blk, wy[...]).astype(BF16)
        rcopy(pm.at[g], yrec.at[g], pm_s.at[g], pm_r.at[g], ep=mate).start()
        blk = spread[2 * g + par]
        pacc[g, :, :C] = dot(blk, wx[...])
        pacc[g, :, C:] = dot(blk, wy[...])

    def pass_on(g):
        rcopy(pm.at[g], yrec.at[g], pm_s.at[g], pm_r.at[g], ep=mate).wait_recv()
        zout[g] = (pacc[g] + yrec[g].astype(F32)).astype(BF16)
        rcopy(zout.at[g], zrec.at[g0], pz_s.at[g], pz_r.at[g0], ep=2 * g + par).start()

    @pl.loop(1, G)
    def _(k):
        g = group(k)
        arrive(2 * g + 1 - par)
        arrive(2 * g + par)
        share(g)

        @pl.when(k > 1)
        def _():
            pass_on(group(k - 1))

    arrive(mate)
    share(g0)
    pass_on(group(G - 1))

    @pl.loop(1, E)
    def _(k):
        s = ep_from(k)
        rcopy(ct.at[s], ctr.at[s], ct_s.at[s], ct_r.at[s], ep=s).wait_recv()

    ctr[e] = ct[e]
    for s in range(E):
        w_ref[s // 2, :, s % 2 * M:(s % 2 + 1) * M] = ctr[s]
    bd[...] = jnp.zeros_like(bd)
    block = ig.shape[1]
    width = bd.shape[1]
    per = width // block
    for i in range(ig.shape[0]):
        lo = i % per * block
        bd[i // per, lo:lo + block, lo:lo + block] = ig[i]
        bd[i // per, lo:lo + block, width + lo:width + lo + block] = dgate[i]
    def before(n):
        row = lax.broadcasted_iota(jnp.int32, (n, n), 0)
        col = lax.broadcasted_iota(jnp.int32, (n, n), 1)
        return ((row < col) & (row // M == col // M)).astype(F32).astype(BF16)

    def rank_of(m, earlier):
        rows = max(16, m.shape[0])
        return dot(jnp.broadcast_to(m, (rows, m.shape[1])).astype(BF16), earlier)[0:1]

    pair = 2 * M
    lower = before(pair)
    slot = lax.broadcasted_iota(jnp.int32, (2 * cap, pair), 0)
    first_slot = lax.broadcasted_iota(jnp.int32, (2 * cap, pair), 1) // M * cap
    slot = (slot - first_slot).astype(F32)

    @pl.loop(0, G)
    def _(g):
        w_row = w_ref[g]
        m = (w_row > 0.0).astype(F32)
        hit = (slot == rank_of(m, lower)).astype(F32) * m
        sel[g] = hit.astype(BF16)
        w_slot[g] = jnp.broadcast_to(jnp.sum(hit * w_row, axis=1, keepdims=True), w_slot.shape[1:])

    lower = before(M)
    slot = lax.broadcasted_iota(jnp.int32, (cap, M), 0).astype(F32)

    def own_hit(p):
        m = (ct[p] > 0.0).astype(F32)
        return (slot == rank_of(m, lower)).astype(F32) * m

    @pl.loop(0, G)
    def _(g):
        own_sel[g] = jnp.concatenate([own_hit(2 * g), own_hit(2 * g + 1)], axis=0).astype(BF16)

    rcopy(pm.at[g0], yrec.at[g0], pm_s.at[g0], pm_r.at[g0], ep=mate).wait_recv()
    acc[...] = pacc[g0] + yrec[g0].astype(F32)

    @pl.loop(1, G)
    def _(k):
        g = group(k)
        rcopy(zout.at[g], zrec.at[g], pz_s.at[g], pz_r.at[g], ep=2 * g + par).wait_recv()
        acc[...] += zrec[g].astype(F32)

    x_b = acc[:, :C].astype(BF16)
    y_b = acc[:, C:].astype(BF16)
    for i in range(1, conv_old.shape[0]):
        conv_new[i - 1] = conv_old[i]
    conv_new[conv_old.shape[0] - 1] = x_b
    conv_pre = conv_old[0].astype(F32) * taps[0:1, :].astype(F32)
    for i in range(1, taps.shape[0] - 1):
        conv_pre = conv_pre + conv_old[i].astype(F32) * taps[i:i + 1, :].astype(F32)
    conv = (conv_pre + x_b.astype(F32) * taps[taps.shape[0] - 1:, :].astype(F32)).astype(BF16)
    gi, gd = [], []
    for i in range(C // width):
        g = dot(conv[:, i * width:(i + 1) * width], bd[i])
        gi.append(g[:, :width])
        gd.append(g[:, width:])
    gate_in = jax.nn.sigmoid(jnp.concatenate(gi, axis=1))
    gate_dec = jax.nn.sigmoid(jnp.concatenate(gd, axis=1))
    dp = decay_param[...]
    log_decay = decay_scale * gate_dec * (jnp.minimum(dp, 0.0) - jnp.log1p(jnp.exp(-jnp.abs(dp))))
    decay = jnp.exp(log_decay)
    inject = jnp.sqrt(-jnp.tanh(log_decay) * (1.0 + decay * decay))
    state = decay * lru[...] + inject * gate_in * conv.astype(F32)
    new_lru[...] = state
    gated = (state * jax.nn.gelu(y_b.astype(F32), approximate=True)).astype(BF16)

    loads[0].wait()
    order = [tp_peer(k) for k in (2, 3, 1)] if T == 4 else [tp_peer(k) for k in range(1, T)]
    for j in order:
        cols = pl.ds(pl.multiple_of(j * C, 128), C)
        mbuf[j] = dot(gated, po[:, cols]).astype(BF16)
        rcopy(mbuf.at[j], mrec.at[t], mx_s.at[j], mx_r.at[t], tp=j).start()
    mixer = dot(gated, po[:, own_cols]).astype(BF16).astype(F32)
    for j in reversed(order):
        rcopy(mbuf.at[j], mrec.at[j], mx_s.at[j], mx_r.at[j], tp=j).wait_recv()
        mixer = mixer + mrec[j].astype(F32)
    summed = (hidden[:, own_cols].astype(F32) + mixer).astype(BF16)
    summed_ref[...] = summed
    sf = summed.astype(F32)
    ssq = jnp.sum(sf * sf, axis=1, keepdims=True)
    same = lax.broadcasted_iota(jnp.int32, (M, M), 0) == lax.broadcasted_iota(jnp.int32, (M, M), 1)
    srow[t, e] = jnp.sum(jnp.where(same, ssq, 0.0), axis=0, keepdims=True)

    def each_other(fn):
        @pl.loop(1, E * T)
        def _(k):
            r = lax.rem(e * T + t + k, E * T)
            fn(r // T, lax.rem(r, T))

    def scale_to(p, q):
        return rcopy(srow.at[t, e], srow.at[t, e], q_s.at[q, p], q_r.at[t, e], ep=p, tp=q)

    each_other(lambda p, q: scale_to(p, q).start())
    xall[t, e] = (sf * ffn_gain[own_cols].reshape(1, C).astype(F32)).astype(BF16)

    core = lax.rem(t, 2)
    to_across = core * (across - t)
    to_mate = (1 - core) * (mate - e)
    first = dict(ep=e + to_mate, tp=t + to_across)
    second = dict(ep=e + core * (mate - e), tp=t + (1 - core) * (across - t))

    def slice_a(k):
        return t, 2 * peer_group(k) + par

    def slice_b(k):
        q, s = slice_a(k)
        return q + to_across, s + (1 - core) * (mate_of(s) - s)

    def slice_c(k):
        q, s = slice_a(k)
        return q + (1 - core) * (across - t), s + core * (mate_of(s) - s)

    def slice_d(k):
        q, s = slice_a(k)
        return across, mate_of(s)

    def move(at, sem, **to):
        q, s = at
        return rcopy(xall.at[q, s], xall.at[q, s], sem, x_r.at[q, s], **to)

    def landed(at):
        move(at, xr_s.at[0], ep=mate).wait_recv()

    def rail(k):
        return move(slice_a(0), xr_s.at[k], ep=2 * peer_group(k) + par)

    def first_a(k):
        return move(slice_a(k), xf_s.at[k], **first)

    def second_a(k):
        return move(slice_a(k), xs_s.at[0, k], **second)

    def second_b(k):
        return move(slice_b(k), xs_s.at[1, k], **second)

    def beside_of(i, k):
        return move((slice_a, slice_b, slice_c, slice_d)[i](k), xd_s.at[i, k], tp=beside)

    def pass_a(k):
        first_a(k).start()
        second_a(k).start()
        beside_of(0, k).start()

    @pl.loop(1, G)
    def _(k):
        rail(k).start()

    pass_a(0)
    own_dw.wait()
    for j in order:
        rcopy(dwp.at[j], dwr.at[j], dw_s.at[j], dw_r.at[j], tp=j).wait_recv()
    square = (
        lax.broadcasted_iota(jnp.int32, (pair, pair), 0) == lax.broadcasted_iota(jnp.int32, (pair, pair), 1)
    )

    def a_copy(q, g, i, to):
        return rcopy(aall.at[q, g], aall.at[q, g], a_s.at[i, g], a_r.at[q, g], tp=to)

    def pair_in(k):
        g = peer_group(k)
        for i in range(2):
            s = 2 * g + i
            total = jnp.zeros((1, M), F32)
            for q in range(T):
                @pl.when((s != e) | (q != t))
                def _():
                    rcopy(srow.at[q, s], srow.at[q, s], q_s.at[q, s], q_r.at[q, s], ep=mate).wait_recv()

                total = total + srow[q, s]
            prow[:, i * M:(i + 1) * M] = total
            landed((beside, s))
            landed((diagonal, s))
        scale_row = lax.rsqrt(prow[...] * (1.0 / D) + epsilon)
        scale = jnp.sum(jnp.where(square, scale_row, 0.0), axis=1, keepdims=True)
        h = None
        for q in range(T):
            part = dot(xall[q, pl.ds(2 * g, 2)].reshape(pair, C), dwr[q])
            h = part if h is None else h + part
        h = h * scale
        half = h.shape[1] // 2
        act = jax.nn.silu(h) * pltpu.roll(h, half, axis=1)
        aall[t, g] = act[:, :half].astype(BF16)
        a_copy(t, g, 0, across).start()
        a_copy(t, g, 1, beside).start()
        pick = sel[g]
        for q in range(T):
            xe[g, :, q * C:(q + 1) * C] = dot(pick, xall[q, pl.ds(2 * g, 2)].reshape(pair, C)).astype(BF16)
        s_slot[g] = jnp.broadcast_to(
            jnp.sum(pick.astype(F32) * scale_row, axis=1, keepdims=True), s_slot.shape[1:]
        )

    def a_forward(k):
        g = peer_group(k)
        a_copy(across, g, 0, across).wait_recv()
        a_copy(across, g, 2, beside).start()

    gate = jax.nn.sigmoid(branch[...])

    def dense(k):
        g = peer_group(k)
        a_copy(beside, g, 1, beside).wait_recv()
        a_copy(diagonal, g, 2, beside).wait_recv()
        d = dot(aall[0, g], dd[0])
        for q in range(1, T):
            d = d + dot(aall[q, g], dd[q])
        dtmp[...] = (d * gate).reshape(2, M, C)
        om[g] = dtmp[1 - par].astype(BF16)
        rcopy(om.at[g], orm.at[g], om_s.at[g], om_r.at[g], ep=mate).start()
        dacc[g] = dtmp[par]

    def dense_on(k):
        g = peer_group(k)
        rcopy(om.at[g], orm.at[g], om_s.at[g], om_r.at[g], ep=mate).wait_recv()
        oz[g] = (dacc[g] + orm[g].astype(F32)).astype(BF16)
        rcopy(oz.at[g], ozr.at[g0], oz_s.at[g], oz_r.at[g0], ep=2 * g + par).start()

    for l in loads[4:5]:
        l.wait()

    @pl.loop(0, G + 2)
    def _(k):
        @pl.when((k >= 1) & (k < G))
        def _():
            landed(slice_a(k))
            pass_a(k)

        @pl.when((k >= 1) & (k <= G))
        def _():
            landed(slice_b(k - 1))
            second_b(k - 1).start()
            beside_of(1, k - 1).start()
            landed(slice_c(k - 1))
            beside_of(2, k - 1).start()

        @pl.when(k >= 2)
        def _():
            landed(slice_d(k - 2))
            beside_of(3, k - 2).start()
            pair_in(k - 2)

        @pl.when(k >= 3)
        def _():
            a_forward(k - 3)

        @pl.when(k >= 4)
        def _():
            dense(k - 4)

    loads[1].wait()
    loads[2].wait()
    FH = eg.shape[1]
    nch = 256 if FH % 256 == 0 else FH
    slots = E * cap

    @pl.loop(0, FH // nch)
    def _(n):
        cols = pl.ds(pl.multiple_of(n * nch, 128), nch)
        rows_in = xe[...].reshape(slots, D)
        scale = s_slot[...].reshape(slots, 128)[:, 0:1]
        g = dot(rows_in, eg[:, cols]) * scale
        u = dot(rows_in, eu[:, cols]) * scale
        hid[:, cols] = (jax.nn.silu(g) * u).astype(BF16)

    loads[3].wait()

    def down(j):
        return dot(hid[...], ed[:, pl.ds(pl.multiple_of(j * C, 128), C)])

    def e_copy(i):
        return rcopy(ebuf.at[i], erec.at[i], ed_s.at[i], ed_r.at[i], tp=beside)

    for i, j in ((1, diagonal), (0, beside)):
        ebuf[i] = down(j).reshape(G, 2 * cap, C).astype(BF16)
        e_copy(i).start()
    epart[1] = down(across).reshape(G, 2 * cap, C)
    epart[0] = down(t).reshape(G, 2 * cap, C)
    a_forward(G - 1)

    def ex_copy(g):
        return rcopy(ex.at[g], exr.at[g], ex_s.at[g], ex_r.at[g], tp=across)

    e_copy(1).wait_recv()

    @pl.loop(0, G)
    def _(k):
        g = peer_group(G - 1 - k)
        ex[g] = (epart[1, g] + erec[1, g].astype(F32)).astype(BF16)
        ex_copy(g).start()

    for k in range(max(0, G - 2), G):
        dense(k)
    e_copy(0).wait_recv()

    @pl.loop(1, G)
    def _(k):
        dense_on(k)


    def eo_copy(s, p):
        return rcopy(eo.at[s], eor.at[p], eo_s.at[s], eo_r.at[p], ep=s)

    @pl.loop(0, G)
    def _(k):
        g = peer_group(G - 1 - k)
        ex_copy(g).wait_recv()
        red = epart[0, g] + erec[0, g].astype(F32) + exr[g].astype(F32)
        red = red.astype(BF16).astype(F32) * w_slot[g][:, 0:1]
        eo[pl.ds(2 * g, 2)] = red.reshape(2, cap, C).astype(BF16)
        for i in range(2):
            s = 2 * g + i

            @pl.when(s != e)
            def _():
                eo_copy(s, e).start()

    eor[e] = eo[e]
    rcopy(om.at[g0], orm.at[g0], om_s.at[g0], om_r.at[g0], ep=mate).wait_recv()
    acc[:, :C] = summed_ref[...].astype(F32) + dacc[g0] + orm[g0].astype(F32)

    @pl.loop(1, G)
    def _(k):
        g = peer_group(k)
        rcopy(oz.at[g], ozr.at[g], oz_s.at[g], oz_r.at[g], ep=2 * g + par).wait_recv()
        acc[:, :C] += ozr[g].astype(F32)


    @pl.loop(1, E)
    def _(k):
        p = ep_from(k)
        eo_copy(p, p).wait_recv()

    picked = eor[...].astype(F32).reshape(slots, C).astype(BF16)
    new_hidden[...] = (
        acc[:, :C] + lax.dot_general(
            own_sel[...].reshape(slots, M), picked, (((0,), (0,)), ((), ())), preferred_element_type=F32
        )
    ).astype(BF16)

    @pl.loop(1, E)
    def _(k):
        p = ep_peer(k)
        rcopy(nb.at[p], spread.at[e], nb_s.at[p], nb_r.at[e], ep=p).wait_send()
        rcopy(ct.at[p], ctr.at[e], ct_s.at[p], ct_r.at[e], ep=p).wait_send()

    @pl.loop(0, G)
    def _(k):
        g = peer_group(k)
        rcopy(pm.at[g], yrec.at[g], pm_s.at[g], pm_r.at[g], ep=mate).wait_send()
        rcopy(om.at[g], orm.at[g], om_s.at[g], om_r.at[g], ep=mate).wait_send()
        first_a(k).wait_send()
        second_a(k).wait_send()
        second_b(k).wait_send()
        for i in range(4):
            beside_of(i, k).wait_send()
        a_copy(t, g, 0, across).wait_send()
        a_copy(t, g, 1, beside).wait_send()
        a_copy(across, g, 2, beside).wait_send()
        ex_copy(g).wait_send()

    @pl.loop(1, G)
    def _(k):
        g = group(k)
        p = 2 * g + par
        rcopy(zout.at[g], zrec.at[g0], pz_s.at[g], pz_r.at[g0], ep=p).wait_send()
        rcopy(oz.at[g], ozr.at[g0], oz_s.at[g], oz_r.at[g0], ep=p).wait_send()
        rail(k).wait_send()

    @pl.loop(1, E)
    def _(k):
        eo_copy(ep_peer(k), e).wait_send()

    each_other(lambda p, q: scale_to(p, q).wait_send())
    for j in order:
        rcopy(dwp.at[j], dwr.at[t], dw_s.at[j], dw_r.at[t], tp=j).wait_send()
        rcopy(mbuf.at[j], mrec.at[t], mx_s.at[j], mx_r.at[t], tp=j).wait_send()
    for i in range(2):
        e_copy(i).wait_send()


def store_kernel(a, b, c, a_out, b_out, c_out, sems):
    copies = [
        pltpu.make_async_copy(src, dst, sems.at[i])
        for i, (src, dst) in enumerate(((a, a_out), (b, b_out), (c, c_out)))
    ]
    for copy in copies:
        copy.start()
    for copy in copies:
        copy.wait()


def on_device(
    hidden, mix_gain, proj_x, proj_y, conv_taps, input_gate, decay_gate, decay_param,
    proj_out, conv_state, lru_state, ffn_gain, routes, route_weights,
    expert_gate, expert_up, expert_down, dense_gate, dense_up, dense_down, branch_gate,
):
    E = lax.axis_size("ep")
    T = lax.axis_size("tp")
    M, D = hidden.shape
    C = D // T
    R = proj_x.shape[0]
    N = E * M
    heads, block = input_gate.shape[:2]
    group = max(1, 128 // block)

    experts = expert_gate.shape[0] * E
    cap = -(-(M * routes.shape[1] // experts + 2) // 8) * 8
    slots = E * cap
    G = E // 2
    h = dense_gate.shape[1] // T
    half = -(-2 * h // 128) * 64

    dd = jnp.pad(dense_down.reshape(T, h, C), ((0, 0), (0, half - h), (0, 0)))
    FH = expert_gate.shape[2]
    vm = pl.BlockSpec(memory_space=pltpu.VMEM)
    anyspace = pl.BlockSpec(memory_space=pl.ANY)
    DMA = pltpu.SemaphoreType.DMA
    V = pltpu.VMEM
    scratch = [
        V((E, 1, M), F32), V((G, 1, 2 * M), F32), V((heads // group, group * block, 2 * group * block), BF16),
        V((R, C), BF16), V((R, C), BF16), V((C, T * h), BF16), V((C, T * h), BF16),
        V((C, D), BF16), V((D, FH), BF16), V((D, FH), BF16), V((FH, D), BF16), V((T, half, C), BF16),
        V((E, M, R), BF16), V((T, C, 2 * half), BF16), V((T, C, 2 * half), BF16),
        V((E, M, R), BF16), V((G, M, 2 * C), BF16), V((G, M, 2 * C), F32), V((G, M, 2 * C), BF16),
        V((G, M, 2 * C), BF16), V((G, M, 2 * C), BF16), V((E, 1, M), F32), V((M, 2 * C), F32),
        V((T, M, C), BF16), V((T, M, C), BF16), V((T, E, 1, M), F32), V((1, 2 * M), F32),
        V((T, E, M, C), BF16), V((T, G, 2 * M, half), BF16),
        V((G, 2 * cap, D), BF16), V((slots, FH), BF16), V((G, 2 * cap, 2 * M), BF16),
        V((G, 2 * cap, M), BF16), V((G, 2 * cap, 128), F32), V((G, 2 * cap, 128), F32),
        V((2, G, 2 * cap, C), BF16), V((2, G, 2 * cap, C), BF16), V((2, G, 2 * cap, C), F32),
        V((G, 2 * cap, C), BF16), V((G, 2 * cap, C), BF16), V((E, cap, C), BF16), V((E, cap, C), BF16),
        V((2, M, C), F32),
        V((G, M, C), BF16), V((G, M, C), F32), V((G, M, C), BF16), V((G, M, C), BF16), V((G, M, C), BF16),
        V((M, C), BF16),
        DMA((10,)),
        DMA((E,)), DMA((E,)), DMA((E,)), DMA((E,)), DMA((G,)), DMA((G,)), DMA((G,)), DMA((G,)),
        DMA((T,)), DMA((T,)), DMA((T,)), DMA((T,)), DMA((T, E)), DMA((T, E)),
        DMA((G,)), DMA((G,)), DMA((2, G)), DMA((4, G)), DMA((T, E)), DMA((3, G)), DMA((T, G)),
        DMA((2,)), DMA((2,)), DMA((G,)), DMA((G,)), DMA((E,)), DMA((E,)),
        DMA((G,)), DMA((G,)), DMA((G,)), DMA((G,)),
    ]
    outs = pl.pallas_call(
        functools.partial(layer_kernel, E, T, cap),
        out_shape=(
            jax.ShapeDtypeStruct((M, C), BF16),
            jax.ShapeDtypeStruct((M, C), F32),
            jax.ShapeDtypeStruct((conv_state.shape[1], M, C), BF16),
        ),
        in_specs=[vm] * 12 + [anyspace] * 9,
        out_specs=(vm, vm, vm),
        scratch_shapes=scratch,
        compiler_params=pltpu.CompilerParams(
            collective_id=0, has_side_effects=True, vmem_limit_bytes=60 * 1024 * 1024
        ),
    )(
        hidden, mix_gain, routes.T, route_weights.T, conv_state.transpose(1, 0, 2), conv_taps,
        input_gate, decay_gate, decay_param[None, :], lru_state,
        ffn_gain, branch_gate[None, :],
        proj_x, proj_y, dense_gate, dense_up, proj_out, expert_gate[0], expert_up[0], expert_down[0], dd,
    )
    new_hidden, new_lru, new_conv = pl.pallas_call(
        store_kernel,
        out_shape=tuple(jax.ShapeDtypeStruct(o.shape, o.dtype) for o in outs),
        in_specs=[vm] * 3,
        out_specs=(anyspace,) * 3,
        scratch_shapes=[DMA((3,))],
    )(*outs)
    return (new_hidden, new_lru, new_conv.transpose(1, 0, 2))


def solution(mesh):
    in_specs = (
        P("ep", None),
        P(),
        P("ep", "tp"),
        P("ep", "tp"),
        P(None, "tp"),
        P("tp", None, None),
        P("tp", None, None),
        P("tp"),
        P("tp", None),
        P("ep", None, "tp"),
        P("ep", "tp"),
        P(),
        P("ep", None),
        P("ep", None),
        P("ep", None, "tp"),
        P("ep", None, "tp"),
        P("ep", "tp", None),
        P("tp", "ep"),
        P("tp", "ep"),
        P("ep", "tp"),
        P("tp"),
    )
    out_specs = (P("ep", "tp"), P("ep", "tp"), P("ep", None, "tp"))
    return jax.shard_map(
        on_device, mesh=mesh, in_specs=in_specs, out_specs=out_specs, check_vma=False
    )
```

```python
import functools

import jax
import jax.numpy as jnp
from jax import lax
from jax.experimental import pallas as pl
from jax.experimental.pallas import tpu as pltpu
from jax.sharding import PartitionSpec as P

epsilon = 1e-06
decay_scale = 8.0
MESH = pl.DeviceIdType.MESH
F32 = jnp.float32
BF16 = jnp.bfloat16


def dot(a, b):
    return jnp.dot(a, b, preferred_element_type=F32)


def layer_kernel(
    E, T, cap,
    hidden, mix_gain, routes, weights, conv_old, taps, ig, dgate, decay_param, lru, ffn_gain, branch,
    wx_h, wy_h, dg_h, du_h, po_h, eg_h, eu_h, ed_h, dd_h,
    new_hidden, new_lru, conv_new,
    ct, w_ref, bd, wall, dg, du, po, eg, eu, ed, dd, nb, dwp, dwr, xin, zf, zout, zrec, ctr, acc,
    mbuf, mrec, srow, prow, xall, aall, xe, hid, sel, own_sel, w_slot, s_slot,
    ebuf, erec, epart, ex, exr, eo, eor, dtmp, om, dacc, orm, oz, ozr, summed_ref,
    load_sem, w_l, w_s, w_r, nb_s, nb_r, nf_s, nf_r, ct_s, ct_r, pz_s, pz_r, dw_s, dw_r, mx_s, mx_r, q_s, q_r,
    x_s, x_r, xb_r, a_s, a_r, ab_r, ed_s, ed_r, ex_s, ex_r, eo_s, eo_r, om_s, om_r, oz_s, oz_r,
):
    e = lax.axis_index("ep")
    t = lax.axis_index("tp")
    M, D = hidden.shape
    C = D // T
    R = wx_h.shape[0]
    chunks, CW = wall.shape[0], wall.shape[3]
    G = E // 2
    g0 = e // 2
    par = lax.rem(e, 2)
    mate = e + 1 - 2 * par
    own_cols = pl.ds(pl.multiple_of(t * C, 128), C)

    def ep_peer(k):
        return lax.rem(e + k, E)

    def ep_from(k):
        return lax.rem(e + E - k, E)

    def group(k):
        return lax.rem(g0 + k, G)

    def rail_from(k):
        return 2 * lax.rem(g0 + G - k, G) + par

    def mate_of(s):
        return s + 1 - 2 * lax.rem(s, 2)

    def peer_group(k):
        if G & (G - 1):
            return lax.rem(g0 + k, G)
        g, bit = 0, 1
        while bit < G:
            g = g + bit * lax.rem(g0 // bit + k // bit, 2)
            bit *= 2
        return g

    def tp_peer(k):
        return lax.rem(t + k, T)

    across = lax.rem(t + T // 2, T)
    beside = t + 1 - 2 * lax.rem(t, 2)
    diagonal = lax.rem(beside + T // 2, T)

    loads = [
        pltpu.make_async_copy(src, dst, load_sem.at[i])
        for i, (src, dst) in enumerate(
            ((po_h, po), (eg_h, eg), (eu_h, eu), (ed_h, ed), (dd_h, dd),
             (dg_h, dg), (du_h, du))
        )
    ]
    own_dw = pltpu.make_async_copy(dwp.at[t], dwr.at[t], load_sem.at[7])

    def w_load(i):
        src, col = (wx_h, i * CW) if i * CW < C else (wy_h, i * CW - C)
        return pltpu.make_async_copy(src.at[:, pl.ds(col, CW)], wall.at[i, par], w_l.at[0])

    for i in range(chunks):
        w_load(i).start()
    for i in (5, 6, 0):
        loads[i].start()

    def rcopy(src, dst, s, r, ep=None, tp=None):
        return pltpu.make_async_remote_copy(
            src_ref=src, dst_ref=dst, send_sem=s, recv_sem=r,
            device_id=(e if ep is None else ep, t if tp is None else tp),
            device_id_type=MESH,
        )

    barrier = pltpu.get_barrier_semaphore()

    @pl.loop(1, E)
    def _(k):
        pl.semaphore_signal(barrier, inc=1, device_id=(ep_peer(k), t), device_id_type=MESH)

    for k in range(1, T):
        pl.semaphore_signal(barrier, inc=1, device_id=(e, tp_peer(k)), device_id_type=MESH)
    hf = hidden[...].astype(F32)
    inv = lax.rsqrt(jnp.mean(hf * hf, axis=-1, keepdims=True) + epsilon)
    normed = (hf * inv * mix_gain[...].reshape(1, D).astype(F32)).astype(BF16)
    for g in range(G):
        nb[g] = normed[:, 2 * g * R:2 * (g + 1) * R].reshape(2, M // 2, 2 * R)
    for p in range(E):
        ct[p] = jnp.sum(jnp.where(routes[...] == p, weights[...], 0.0), axis=0, keepdims=True)
    pl.semaphore_wait(barrier, E - 1 + T - 1)

    core = lax.rem(t, 2)

    def w_copy(i):
        return rcopy(wall.at[i, par], wall.at[i, par], w_s.at[0], w_r.at[i], ep=mate)

    def w_in(i):
        return rcopy(wall.at[i, 1 - par], wall.at[i, 1 - par], w_s.at[0], w_r.at[i], ep=mate)

    def nb_copy(g):
        return rcopy(nb.at[g, core], xin.at[g0, core], nb_s.at[0], nb_r.at[g0], ep=2 * g + par)

    def nb_in(g):
        return rcopy(nb.at[g, core], xin.at[g, core], nb_s.at[0], nb_r.at[g], ep=mate)

    def nb_beside(g):
        return rcopy(xin.at[g, core], xin.at[g, core], nf_s.at[0], nf_r.at[0], tp=beside)

    rest = pl.ds(0, G - 1)

    @pl.loop(1, E)
    def _(k):
        p = ep_peer(k)
        rcopy(ct.at[p], ctr.at[e], ct_s.at[0], ct_r.at[0], ep=p).start()

    @pl.loop(1, G)
    def _(k):
        nb_copy(peer_group(k)).start()

    pltpu.make_async_copy(wall.at[:, par], wall.at[:, par], w_l.at[0]).wait()
    for i in range(chunks):
        w_copy(i).start()

    loads[5].wait()
    loads[6].wait()
    h = dg.shape[1] // T
    half = dwp.shape[2] // 2
    if half != h:
        dwp[...] = jnp.zeros_like(dwp)
    for j in range(T):
        dwp[j, :, :h] = dg[:, j * h:(j + 1) * h]
        dwp[j, :, half:half + h] = du[:, j * h:(j + 1) * h]
    own_dw.start()
    for k in range(1, T):
        j = tp_peer(k)
        rcopy(dwp.at[j], dwr.at[t], dw_s.at[0], dw_r.at[0], tp=j).start()
    for l in loads[1:5]:
        l.start()

    xin[g0] = nb[g0]

    @pl.loop(1, G)
    def _(k):
        g = peer_group(k)
        nb_in(g).wait_recv()
        nb_beside(g).start()

    others = pl.ds(0, E - 1)
    ct_all = rcopy(ct.at[others], ctr.at[others], ct_s.at[0], ct_r.at[0], ep=mate)
    ct_all.wait_recv()

    ctr[e] = ct[e]
    for s in range(E):
        w_ref[s // 2, :, s % 2 * M:(s % 2 + 1) * M] = ctr[s]
    bd[...] = jnp.zeros_like(bd)
    block = ig.shape[1]
    width = bd.shape[1]
    per = width // block
    for i in range(ig.shape[0]):
        lo = i % per * block
        bd[i // per, lo:lo + block, lo:lo + block] = ig[i]
        bd[i // per, lo:lo + block, width + lo:width + lo + block] = dgate[i]
    def before(n):
        row = lax.broadcasted_iota(jnp.int32, (n, n), 0)
        col = lax.broadcasted_iota(jnp.int32, (n, n), 1)
        return ((row < col) & (row // M == col // M)).astype(F32).astype(BF16)

    def rank_of(m, earlier):
        rows = max(16, m.shape[0])
        return dot(jnp.broadcast_to(m, (rows, m.shape[1])).astype(BF16), earlier)[0:1]

    pair = 2 * M
    lower = before(pair)
    slot = lax.broadcasted_iota(jnp.int32, (2 * cap, pair), 0)
    first_slot = lax.broadcasted_iota(jnp.int32, (2 * cap, pair), 1) // M * cap
    slot = (slot - first_slot).astype(F32)

    @pl.loop(0, G)
    def _(g):
        w_row = w_ref[g]
        m = (w_row > 0.0).astype(F32)
        hit = (slot == rank_of(m, lower)).astype(F32) * m
        sel[g] = hit.astype(BF16)
        w_slot[g] = jnp.broadcast_to(jnp.sum(hit * w_row, axis=1, keepdims=True), w_slot.shape[1:])

    lower = before(M)
    slot = lax.broadcasted_iota(jnp.int32, (cap, M), 0).astype(F32)

    def own_hit(p):
        m = (ct[p] > 0.0).astype(F32)
        return (slot == rank_of(m, lower)).astype(F32) * m

    @pl.loop(0, G)
    def _(g):
        own_sel[g] = jnp.concatenate([own_hit(2 * g), own_hit(2 * g + 1)], axis=0).astype(BF16)

    def z_copy(i, g):
        return rcopy(zout.at[i, g], zrec.at[i, g0], pz_s.at[0], pz_r.at[i], ep=2 * g + par)

    def z_in(i):
        return rcopy(zout.at[i, rest], zrec.at[i, rest], pz_s.at[0], pz_r.at[i], ep=mate)

    nb_all = rcopy(xin.at[rest, core], xin.at[rest, core], nf_s.at[0], nf_r.at[0], tp=beside)
    nb_all.wait_recv()
    for i in range(chunks):
        w_in(i).wait_recv()
        z = dot(xin[...].reshape(G * M, 2 * R), wall[i].reshape(2 * R, CW)).reshape(G, M, CW)
        zf[...] = z
        zout[i] = z.astype(BF16)

        @pl.loop(1, G)
        def _(k):
            z_copy(i, peer_group(k)).start()

        acc[:, i * CW:(i + 1) * CW] = zf[g0]

    for i in range(chunks):
        z_in(i).wait_recv()

        @pl.loop(1, G)
        def _(k):
            g = peer_group(k)
            acc[:, i * CW:(i + 1) * CW] += zrec[i, g].astype(F32)

    x_b = acc[:, :C].astype(BF16)
    y_b = acc[:, C:].astype(BF16)
    for i in range(1, conv_old.shape[0]):
        conv_new[i - 1] = conv_old[i]
    conv_new[conv_old.shape[0] - 1] = x_b
    conv_pre = conv_old[0].astype(F32) * taps[0:1, :].astype(F32)
    for i in range(1, taps.shape[0] - 1):
        conv_pre = conv_pre + conv_old[i].astype(F32) * taps[i:i + 1, :].astype(F32)
    conv = (conv_pre + x_b.astype(F32) * taps[taps.shape[0] - 1:, :].astype(F32)).astype(BF16)
    gi, gd = [], []
    for i in range(C // width):
        g = dot(conv[:, i * width:(i + 1) * width], bd[i])
        gi.append(g[:, :width])
        gd.append(g[:, width:])
    gate_in = jax.nn.sigmoid(jnp.concatenate(gi, axis=1))
    gate_dec = jax.nn.sigmoid(jnp.concatenate(gd, axis=1))
    dp = decay_param[...]
    log_decay = decay_scale * gate_dec * (jnp.minimum(dp, 0.0) - jnp.log1p(jnp.exp(-jnp.abs(dp))))
    decay = jnp.exp(log_decay)
    inject = jnp.sqrt(-jnp.tanh(log_decay) * (1.0 + decay * decay))
    state = decay * lru[...] + inject * gate_in * conv.astype(F32)
    new_lru[...] = state
    gated = (state * jax.nn.gelu(y_b.astype(F32), approximate=True)).astype(BF16)

    loads[0].wait()
    order = [tp_peer(k) for k in (2, 3, 1)] if T == 4 else [tp_peer(k) for k in range(1, T)]
    for j in order:
        cols = pl.ds(pl.multiple_of(j * C, 128), C)
        mbuf[j] = dot(gated, po[:, cols]).astype(BF16)
        rcopy(mbuf.at[j], mrec.at[t], mx_s.at[0], mx_r.at[0], tp=j).start()
    mixer = dot(gated, po[:, own_cols]).astype(BF16).astype(F32)
    mx_all = rcopy(mbuf.at[pl.ds(0, T - 1)], mrec.at[pl.ds(0, T - 1)], mx_s.at[0], mx_r.at[0], tp=across)
    mx_all.wait_recv()
    for j in order:
        mixer = mixer + mrec[j].astype(F32)
    summed = (hidden[:, own_cols].astype(F32) + mixer).astype(BF16)
    summed_ref[...] = summed
    sf = summed.astype(F32)
    ssq = jnp.sum(sf * sf, axis=1, keepdims=True)
    same = lax.broadcasted_iota(jnp.int32, (M, M), 0) == lax.broadcasted_iota(jnp.int32, (M, M), 1)
    me = t * E + e
    srow[me] = jnp.sum(jnp.where(same, ssq, 0.0), axis=0, keepdims=True)

    def each_other(fn):
        @pl.loop(1, E * T)
        def _(k):
            r = lax.rem(e * T + t + k, E * T)
            fn(r // T, lax.rem(r, T))

    def scale_to(p, q):
        return rcopy(srow.at[me], srow.at[me], q_s.at[0], q_r.at[0], ep=p, tp=q)

    each_other(lambda p, q: scale_to(p, q).start())
    everyone = pl.ds(0, E * T - 1)
    scale_all = rcopy(srow.at[everyone], srow.at[everyone], q_s.at[0], q_r.at[0], tp=across)
    xall[me] = (sf * ffn_gain[own_cols].reshape(1, C).astype(F32)).astype(BF16)

    to_across = core * (across - t)
    to_mate = (1 - core) * (mate - e)
    first = dict(ep=e + to_mate, tp=t + to_across)
    second = dict(ep=e + core * (mate - e), tp=t + (1 - core) * (across - t))

    def slice_a(k):
        return t, 2 * peer_group(k) + par

    def slice_b(k):
        q, s = slice_a(k)
        return q + to_across, s + (1 - core) * (mate_of(s) - s)

    def slice_c(k):
        q, s = slice_a(k)
        return q + (1 - core) * (across - t), s + core * (mate_of(s) - s)

    def slice_d(k):
        q, s = slice_a(k)
        return across, mate_of(s)

    def move(at, r, **to):
        q, s = at
        return rcopy(xall.at[q * E + s], xall.at[q * E + s], x_s.at[0], r, **to)

    def landed(i, k):
        move(slice_a(k), x_r.at[i, peer_group(k)], ep=mate).wait_recv()

    def rail_a(k):
        return move(slice_a(0), x_r.at[0, g0], ep=2 * peer_group(k) + par)

    def rail_b(k):
        return move(slice_b(0), x_r.at[1, g0], ep=2 * peer_group(k) + par)

    def first_a(k):
        return move(slice_a(k), x_r.at[1, peer_group(k)], **first)

    def second_a(k):
        return move(slice_a(k), x_r.at[2, peer_group(k)], **second)

    def second_b(k):
        return move(slice_b(k), x_r.at[3, peer_group(k)], **second)

    def beside_of(i, k):
        return move((slice_a, slice_b, slice_c, slice_d)[i](k), xb_r.at[peer_group(k)], tp=beside)

    def pass_on(i, k):
        if i == 0:
            second_a(k).start()
        if i == 1:
            second_b(k).start()
        beside_of(i, k).start()

    first_a(0).start()

    @pl.loop(1, G)
    def _(k):
        rail_a(k).start()

    pass_on(0, 0)
    own_dw.wait()
    peers = pl.ds(0, T - 1)
    dw_all = rcopy(dwp.at[peers], dwr.at[peers], dw_s.at[0], dw_r.at[0], tp=across)
    dw_all.wait_recv()
    square = (
        lax.broadcasted_iota(jnp.int32, (pair, pair), 0) == lax.broadcasted_iota(jnp.int32, (pair, pair), 1)
    )

    def a_copy(q, g, r, to):
        return rcopy(aall.at[q, g], aall.at[q, g], a_s.at[0], r.at[g], tp=to)

    def pair_in(k):
        g = peer_group(k)
        for i in range(2):
            s = 2 * g + i
            total = jnp.zeros((1, M), F32)
            for q in range(T):
                total = total + srow[q * E + s]
            prow[:, i * M:(i + 1) * M] = total
        rcopy(xall.at[pl.ds(0, 4)], xall.at[pl.ds(0, 4)], x_s.at[0], xb_r.at[g], tp=beside).wait_recv()
        scale_row = lax.rsqrt(prow[...] * (1.0 / D) + epsilon)
        scale = jnp.sum(jnp.where(square, scale_row, 0.0), axis=1, keepdims=True)
        h = None
        for q in range(T):
            part = dot(xall[pl.ds(q * E + 2 * g, 2)].reshape(pair, C), dwr[q])
            h = part if h is None else h + part
        h = h * scale
        half = h.shape[1] // 2
        act = jax.nn.silu(h) * pltpu.roll(h, half, axis=1)
        aall[t, g] = act[:, :half].astype(BF16)
        a_copy(t, g, a_r, across).start()
        a_copy(t, g, ab_r, beside).start()
        pick = sel[g]
        for q in range(T):
            xe[g, :, q * C:(q + 1) * C] = dot(pick, xall[pl.ds(q * E + 2 * g, 2)].reshape(pair, C)).astype(BF16)
        s_slot[g] = jnp.broadcast_to(
            jnp.sum(pick.astype(F32) * scale_row, axis=1, keepdims=True), s_slot.shape[1:]
        )

    def a_forward(k):
        g = peer_group(k)
        a_copy(across, g, a_r, across).wait_recv()
        a_copy(across, g, ab_r, beside).start()

    gate = jax.nn.sigmoid(branch[...])

    def dense(k):
        g = peer_group(k)
        rcopy(aall.at[pl.ds(0, 2), g], aall.at[pl.ds(0, 2), g], a_s.at[0], ab_r.at[g], tp=beside).wait_recv()
        d = dot(aall[0, g], dd[0])
        for q in range(1, T):
            d = d + dot(aall[q, g], dd[q])
        dtmp[...] = (d * gate).reshape(2, M, C)
        om[g] = dtmp[1 - par].astype(BF16)
        rcopy(om.at[g], orm.at[g], om_s.at[0], om_r.at[g], ep=mate).start()
        dacc[g] = dtmp[par]

    def dense_on(k):
        g = peer_group(k)
        rcopy(om.at[g], orm.at[g], om_s.at[0], om_r.at[g], ep=mate).wait_recv()
        oz[g] = (dacc[g] + orm[g].astype(F32)).astype(BF16)
        rcopy(oz.at[g], ozr.at[g0], oz_s.at[0], oz_r.at[0], ep=2 * g + par).start()

    for l in loads[4:5]:
        l.wait()

    lag = 2

    @pl.loop(0, G + lag)
    def _(k):
        @pl.when((k >= 1) & (k < G))
        def _():
            landed(0, k)

            @pl.when(core == 0)
            def _():
                first_a(k).start()

            pass_on(0, k)

        @pl.when((k >= 1) & (k <= G))
        def _():
            landed(1, k - 1)

            @pl.when((core == 1) & (k == 1))
            def _():
                @pl.loop(1, G)
                def _(j):
                    rail_b(j).start()

            pass_on(1, k - 1)
            landed(2, k - 1)
            pass_on(2, k - 1)

        @pl.when((k >= 2) & (k <= G + 1))
        def _():
            landed(3, k - 2)
            pass_on(3, k - 2)

        @pl.when(k == lag)
        def _():
            scale_all.wait_recv()

        @pl.when(k >= lag)
        def _():
            pair_in(k - lag)

        @pl.when(k >= lag + 1)
        def _():
            a_forward(k - lag - 1)

        @pl.when(k >= lag + 2)
        def _():
            dense(k - lag - 2)

        @pl.when(k >= lag + 4)
        def _():
            dense_on(k - lag - 3)

    loads[1].wait()
    loads[2].wait()
    FH = eg.shape[1]
    nch = 256 if FH % 256 == 0 else FH
    slots = E * cap

    @pl.loop(0, FH // nch)
    def _(n):
        cols = pl.ds(pl.multiple_of(n * nch, 128), nch)
        rows_in = xe[...].reshape(slots, D)
        scale = s_slot[...].reshape(slots, 128)[:, 0:1]
        g = dot(rows_in, eg[:, cols]) * scale
        u = dot(rows_in, eu[:, cols]) * scale
        hid[:, cols] = (jax.nn.silu(g) * u).astype(BF16)

    loads[3].wait()

    def down(j):
        return dot(hid[...], ed[:, pl.ds(pl.multiple_of(j * C, 128), C)])

    def e_copy(i):
        return rcopy(ebuf.at[i], erec.at[i], ed_s.at[0], ed_r.at[i], tp=beside)

    def ex_copy(g):
        return rcopy(ex.at[g], exr.at[g], ex_s.at[0], ex_r.at[g], tp=across)

    def eo_copy(s, p):
        return rcopy(eo.at[s], eor.at[p], eo_s.at[0], eo_r.at[0], ep=s)

    def ex_out(k):
        g = peer_group(k)
        ex[g] = (epart[1, g] + erec[1, g].astype(F32)).astype(BF16)
        ex_copy(g).start()

    def ex_in(k):
        g = peer_group(k)
        ex_copy(g).wait_recv()
        red = epart[0, g] + erec[0, g].astype(F32) + exr[g].astype(F32)
        red = red.astype(BF16).astype(F32) * w_slot[g][:, 0:1]
        eo[pl.ds(2 * g, 2)] = red.reshape(2, cap, C).astype(BF16)
        for i in range(2):
            s = 2 * g + i

            @pl.when(s != e)
            def _():
                eo_copy(s, e).start()

    for i, j in ((1, diagonal), (0, beside)):
        ebuf[i] = down(j).reshape(G, 2 * cap, C).astype(BF16)
        e_copy(i).start()
    a_forward(G - 1)
    epart[1] = down(across).reshape(G, 2 * cap, C)
    epart[0] = down(t).reshape(G, 2 * cap, C)
    e_copy(1).wait_recv()

    @pl.loop(0, G)
    def _(k):
        ex_out(G - 1 - k)

    if G > 1:
        dense(G - 2)
    if G > 3:
        dense_on(G - 3)
    dense(G - 1)
    if G > 2:
        dense_on(G - 2)
    e_copy(0).wait_recv()
    ex_in(G - 1)
    if G > 1:
        dense_on(G - 1)

    @pl.loop(1, G)
    def _(k):
        ex_in(G - 1 - k)

    eor[e] = eo[e]
    rcopy(om.at[g0], orm.at[g0], om_s.at[0], om_r.at[g0], ep=mate).wait_recv()
    acc[:, :C] = summed_ref[...].astype(F32) + dacc[g0] + orm[g0].astype(F32)

    oz_all = rcopy(oz.at[rest], ozr.at[rest], oz_s.at[0], oz_r.at[0], ep=mate)
    oz_all.wait_recv()

    @pl.loop(1, G)
    def _(k):
        g = peer_group(k)
        acc[:, :C] += ozr[g].astype(F32)


    eo_all = rcopy(eo.at[others], eor.at[others], eo_s.at[0], eo_r.at[0], ep=mate)
    eo_all.wait_recv()

    picked = eor[...].astype(F32).reshape(slots, C).astype(BF16)
    new_hidden[...] = (
        acc[:, :C] + lax.dot_general(
            own_sel[...].reshape(slots, M), picked, (((0,), (0,)), ((), ())), preferred_element_type=F32
        )
    ).astype(BF16)
    for copy in (ct_all, nb_all, dw_all, mx_all, scale_all, oz_all, eo_all):
        copy.wait_send()
    z_all = zout.at[:, rest]
    for ref, sem in (
        (wall.at[:, par], w_s), (nb.at[rest, core], nb_s), (z_all, pz_s), (xall.at[everyone], x_s),
        (aall.at[pl.ds(0, 3)], a_s), (ebuf, ed_s), (ex, ex_s), (om, om_s),
    ):
        rcopy(ref, ref, sem.at[0], sem.at[0], tp=across).wait_send()


def store_kernel(a, b, c, a_out, b_out, c_out, sems):
    copies = [
        pltpu.make_async_copy(src, dst, sems.at[i])
        for i, (src, dst) in enumerate(((a, a_out), (b, b_out), (c, c_out)))
    ]
    for copy in copies:
        copy.start()
    for copy in copies:
        copy.wait()


def on_device(
    hidden, mix_gain, proj_x, proj_y, conv_taps, input_gate, decay_gate, decay_param,
    proj_out, conv_state, lru_state, ffn_gain, routes, route_weights,
    expert_gate, expert_up, expert_down, dense_gate, dense_up, dense_down, branch_gate,
):
    E = lax.axis_size("ep")
    T = lax.axis_size("tp")
    M, D = hidden.shape
    C = D // T
    R = proj_x.shape[0]
    N = E * M
    heads, block = input_gate.shape[:2]
    group = max(1, 128 // block)

    experts = expert_gate.shape[0] * E
    cap = -(-(M * routes.shape[1] // experts + 2) // 8) * 8
    slots = E * cap
    G = E // 2
    h = dense_gate.shape[1] // T
    half = -(-2 * h // 128) * 64

    dd = jnp.pad(dense_down.reshape(T, h, C), ((0, 0), (0, half - h), (0, 0)))
    FH = expert_gate.shape[2]
    vm = pl.BlockSpec(memory_space=pltpu.VMEM)
    anyspace = pl.BlockSpec(memory_space=pl.ANY)
    DMA = pltpu.SemaphoreType.DMA
    V = pltpu.VMEM
    chunks = max(1, 2 * C // 128)
    scratch = [
        V((E, 1, M), F32), V((G, 1, 2 * M), F32), V((heads // group, group * block, 2 * group * block), BF16),
        V((chunks, 2, R, 2 * C // chunks), BF16), V((C, T * h), BF16), V((C, T * h), BF16),
        V((C, D), BF16), V((D, FH), BF16), V((D, FH), BF16), V((FH, D), BF16), V((T, half, C), BF16),
        V((G, 2, M // 2, 2 * R), BF16), V((T, C, 2 * half), BF16), V((T, C, 2 * half), BF16),
        V((G, 2, M // 2, 2 * R), BF16), V((G, M, 2 * C // chunks), F32),
        V((chunks, G, M, 2 * C // chunks), BF16), V((chunks, G, M, 2 * C // chunks), BF16),
        V((E, 1, M), F32), V((M, 2 * C), F32),
        V((T, M, C), BF16), V((T, M, C), BF16), V((T * E, 1, M), F32), V((1, 2 * M), F32),
        V((T * E, M, C), BF16), V((T, G, 2 * M, half), BF16),
        V((G, 2 * cap, D), BF16), V((slots, FH), BF16), V((G, 2 * cap, 2 * M), BF16),
        V((G, 2 * cap, M), BF16), V((G, 2 * cap, 128), F32), V((G, 2 * cap, 128), F32),
        V((2, G, 2 * cap, C), BF16), V((2, G, 2 * cap, C), BF16), V((2, G, 2 * cap, C), F32),
        V((G, 2 * cap, C), BF16), V((G, 2 * cap, C), BF16), V((E, cap, C), BF16), V((E, cap, C), BF16),
        V((2, M, C), F32),
        V((G, M, C), BF16), V((G, M, C), F32), V((G, M, C), BF16), V((G, M, C), BF16), V((G, M, C), BF16),
        V((M, C), BF16),
        DMA((8,)), DMA((1,)), DMA((1,)), DMA((chunks,)),
        DMA((1,)), DMA((G,)), DMA((1,)), DMA((1,)), DMA((1,)), DMA((1,)), DMA((1,)), DMA((chunks,)),
        DMA((1,)), DMA((1,)), DMA((1,)), DMA((1,)), DMA((1,)), DMA((1,)),
        DMA((1,)), DMA((4, G)), DMA((G,)), DMA((1,)), DMA((G,)), DMA((G,)),
        DMA((1,)), DMA((2,)), DMA((1,)), DMA((G,)), DMA((1,)), DMA((1,)),
        DMA((1,)), DMA((G,)), DMA((1,)), DMA((1,)),
    ]
    outs = pl.pallas_call(
        functools.partial(layer_kernel, E, T, cap),
        out_shape=(V((M, C), BF16), V((M, C), F32), V((conv_state.shape[1], M, C), BF16)),
        in_specs=[vm] * 12 + [anyspace] * 9,
        out_specs=(vm, vm, vm),
        scratch_shapes=scratch,
        compiler_params=pltpu.CompilerParams(
            collective_id=0, has_side_effects=True, vmem_limit_bytes=60 * 1024 * 1024
        ),
    )(
        hidden, mix_gain, routes.T, route_weights.T, conv_state.transpose(1, 0, 2), conv_taps,
        input_gate, decay_gate, decay_param[None, :], lru_state,
        ffn_gain, branch_gate[None, :],
        proj_x, proj_y, dense_gate, dense_up, proj_out, expert_gate[0], expert_up[0], expert_down[0], dd,
    )
    new_hidden, new_lru, new_conv = pl.pallas_call(
        store_kernel,
        out_shape=tuple(jax.ShapeDtypeStruct(o.shape, o.dtype) for o in outs),
        in_specs=[vm] * 3,
        out_specs=(anyspace,) * 3,
        scratch_shapes=[DMA((3,))],
    )(*(pltpu.with_memory_space_constraint(o, pltpu.VMEM) for o in outs))
    return (new_hidden, new_lru, new_conv.transpose(1, 0, 2))


def solution(mesh):
    in_specs = (
        P("ep", None),
        P(),
        P("ep", "tp"),
        P("ep", "tp"),
        P(None, "tp"),
        P("tp", None, None),
        P("tp", None, None),
        P("tp"),
        P("tp", None),
        P("ep", None, "tp"),
        P("ep", "tp"),
        P(),
        P("ep", None),
        P("ep", None),
        P("ep", None, "tp"),
        P("ep", None, "tp"),
        P("ep", "tp", None),
        P("tp", "ep"),
        P("tp", "ep"),
        P("ep", "tp"),
        P("tp"),
    )
    out_specs = (P("ep", "tp"), P("ep", "tp"), P("ep", None, "tp"))
    return jax.shard_map(
        on_device, mesh=mesh, in_specs=in_specs, out_specs=out_specs, check_vma=False
    )
```

```python
import functools

import jax
import jax.numpy as jnp
from jax import lax
from jax.experimental import pallas as pl
from jax.experimental.pallas import tpu as pltpu
from jax.sharding import PartitionSpec as P

epsilon = 1e-06
decay_scale = 8.0
MESH = pl.DeviceIdType.MESH
DIRECT = 3
F32 = jnp.float32
BF16 = jnp.bfloat16


def dot(a, b):
    return jnp.dot(a, b, preferred_element_type=F32)


def layer_kernel(
    E, T, cap,
    hidden_h, mix_gain_h, routes_h, weights_h, conv_old_h, taps_h, ig_h, dgate_h, decay_param_h, lru_h,
    ffn_gain_h, branch_h,
    wx_h, wy_h, dg_h, du_h, po_h, eg_h, eu_h, ed_h, dd_h,
    new_hidden, new_lru, conv_new,
    hidden, mix_gain, routes, weights, conv_old, taps, ig, dgate, decay_param, lru, ffn_gain, branch,
    ct, w_ref, bd, wall, dg, du, po, eg, eu, ed, dd, nb, dwp, dwr, xin, zf, zlast, zpair, zout, zrec, ctr, acc,
    mbuf, mrec, srow, stot, prow, xall, aall, xe, hid, sel, own_sel, w_slot, s_slot,
    ebuf, erec, epart, ex, exr, eo, eor, dtmp, om, dacc, orm, oz, ozr, ozx, summed_ref,
    load_sem, in_l, w_l, w_s, w_r, nb_s, nb_r, nf_s, nf_r, ct_s, ct_r, pz_s, pz_r, zx_r, dw_s, dw_r, mx_s, mx_r, q_s, q_r, qe_s, qe_r,
    x_s, x_r, xb_r, a_s, a_r, ab_r, ed_s, ed_r, ex_s, ex_r, eo_s, eo_r, om_s, om_r, oz_s, oz_r, ozx_r, ozf_r,
):
    e = lax.axis_index("ep")
    t = lax.axis_index("tp")
    M, D = hidden.shape
    C = D // T
    R = wx_h.shape[0]
    chunks, CW = wall.shape[0], wall.shape[3]
    G = E // 2
    g0 = e // 2
    par = lax.rem(e, 2)
    mate = e + 1 - 2 * par
    own_cols = pl.ds(pl.multiple_of(t * C, 128), C)

    def ep_peer(k):
        return lax.rem(e + k, E)

    def ep_from(k):
        return lax.rem(e + E - k, E)

    def group(k):
        return lax.rem(g0 + k, G)

    def rail_from(k):
        return 2 * lax.rem(g0 + G - k, G) + par

    def mate_of(s):
        return s + 1 - 2 * lax.rem(s, 2)

    upper = G // 2
    paired = G > 2 and G & (G - 1) == 0

    def flip(g, mask):
        out, bit = 0, 1
        while bit < G:
            out = out + bit * lax.rem(g // bit + mask // bit, 2)
            bit *= 2
        return out

    def peer_group(k):
        if not paired:
            return lax.rem(g0 + k, G)
        return flip(g0, k // upper * upper + lax.rem(k + k // upper, upper))

    def tp_peer(k):
        return lax.rem(t + k, T)

    across = lax.rem(t + T // 2, T)
    beside = t + 1 - 2 * lax.rem(t, 2)
    diagonal = lax.rem(beside + T // 2, T)

    inputs = [
        pltpu.make_async_copy(src, dst, in_l.at[i])
        for i, (src, dst) in enumerate(
            ((hidden_h, hidden), (mix_gain_h, mix_gain), (routes_h, routes), (weights_h, weights),
             (conv_old_h, conv_old), (taps_h, taps), (ig_h, ig), (dgate_h, dgate),
             (decay_param_h, decay_param), (lru_h, lru), (ffn_gain_h, ffn_gain), (branch_h, branch))
        )
    ]
    for copy in inputs[:4]:
        copy.start()

    barrier = pltpu.get_barrier_semaphore()

    @pl.loop(1, E)
    def _(k):
        pl.semaphore_signal(barrier, inc=1, device_id=(ep_peer(k), t), device_id_type=MESH)

    for k in range(1, T):
        pl.semaphore_signal(barrier, inc=1, device_id=(e, tp_peer(k)), device_id_type=MESH)

    loads = [
        pltpu.make_async_copy(src, dst, load_sem.at[i])
        for i, (src, dst) in enumerate(
            ((po_h, po), (eg_h, eg), (eu_h, eu), (ed_h, ed), (dd_h, dd),
             (dg_h, dg), (du_h, du))
        )
    ]
    own_dw = pltpu.make_async_copy(dwp.at[t], dwr.at[t], load_sem.at[7])

    def w_load(i):
        src, col = (wx_h, i * CW) if i * CW < C else (wy_h, i * CW - C)
        return pltpu.make_async_copy(src.at[:, pl.ds(col, CW)], wall.at[i, par], w_l.at[0])

    for i in range(chunks):
        w_load(i).start()
    for i in (5, 6, 0):
        loads[i].start()
    for copy in inputs[4:]:
        copy.start()

    def rcopy(src, dst, s, r, ep=None, tp=None):
        return pltpu.make_async_remote_copy(
            src_ref=src, dst_ref=dst, send_sem=s, recv_sem=r,
            device_id=(e if ep is None else ep, t if tp is None else tp),
            device_id_type=MESH,
        )

    for copy in inputs[:4]:
        copy.wait()
    hf = hidden[...].astype(F32)
    inv = lax.rsqrt(jnp.mean(hf * hf, axis=-1, keepdims=True) + epsilon)
    normed = (hf * inv * mix_gain[...].reshape(1, D).astype(F32)).astype(BF16)
    for g in range(G):
        nb[g] = normed[:, 2 * g * R:2 * (g + 1) * R].reshape(2, M // 2, 2 * R)
    for p in range(E):
        ct[p] = jnp.sum(jnp.where(routes[...] == p, weights[...], 0.0), axis=0, keepdims=True)
    pl.semaphore_wait(barrier, E - 1 + T - 1)

    core = lax.rem(t, 2)

    def w_copy(i):
        return rcopy(wall.at[i, par], wall.at[i, par], w_s.at[0], w_r.at[i], ep=mate)

    def w_in(i):
        return rcopy(wall.at[i, 1 - par], wall.at[i, 1 - par], w_s.at[0], w_r.at[i], ep=mate)

    def nb_copy(g):
        return rcopy(nb.at[g, core], xin.at[g0, core], nb_s.at[0], nb_r.at[g0], ep=2 * g + par)

    def nb_in(g):
        return rcopy(nb.at[g, core], xin.at[g, core], nb_s.at[0], nb_r.at[g], ep=mate)

    def nb_beside(g):
        return rcopy(xin.at[g, core], xin.at[g, core], nf_s.at[0], nf_r.at[0], tp=beside)

    rest = pl.ds(0, G - 1)

    @pl.loop(1, E)
    def _(k):
        p = ep_peer(k)
        rcopy(ct.at[p], ctr.at[e], ct_s.at[0], ct_r.at[0], ep=p).start()

    @pl.loop(1, G)
    def _(k):
        nb_copy(peer_group(k)).start()

    pltpu.make_async_copy(wall.at[:, par], wall.at[:, par], w_l.at[0]).wait()
    for i in range(chunks):
        w_copy(i).start()

    loads[5].wait()
    loads[6].wait()
    h = dg.shape[1] // T
    half = dwp.shape[2] // 2
    if half != h:
        dwp[...] = jnp.zeros_like(dwp)
    for j in range(T):
        dwp[j, :, :h] = dg[:, j * h:(j + 1) * h]
        dwp[j, :, half:half + h] = du[:, j * h:(j + 1) * h]
    own_dw.start()
    for k in range(1, T):
        j = tp_peer(k)
        rcopy(dwp.at[j], dwr.at[t], dw_s.at[0], dw_r.at[0], tp=j).start()
    for l in loads[1:5]:
        l.start()

    for copy in inputs[4:]:
        copy.wait()
    xin[g0] = nb[g0]

    @pl.loop(1, G)
    def _(k):
        g = peer_group(k)
        nb_in(g).wait_recv()
        nb_beside(g).start()

    others = pl.ds(0, E - 1)
    ct_all = rcopy(ct.at[others], ctr.at[others], ct_s.at[0], ct_r.at[0], ep=mate)
    ct_all.wait_recv()

    ctr[e] = ct[e]
    for s in range(E):
        w_ref[s // 2, :, s % 2 * M:(s % 2 + 1) * M] = ctr[s]
    bd[...] = jnp.zeros_like(bd)
    block = ig.shape[1]
    width = bd.shape[1]
    per = width // block
    for i in range(ig.shape[0]):
        lo = i % per * block
        bd[i // per, lo:lo + block, lo:lo + block] = ig[i]
        bd[i // per, lo:lo + block, width + lo:width + lo + block] = dgate[i]
    def before(n):
        row = lax.broadcasted_iota(jnp.int32, (n, n), 0)
        col = lax.broadcasted_iota(jnp.int32, (n, n), 1)
        return ((row < col) & (row // M == col // M)).astype(F32).astype(BF16)

    def rank_of(m, earlier):
        rows = max(16, m.shape[0])
        return dot(jnp.broadcast_to(m, (rows, m.shape[1])).astype(BF16), earlier)[0:1]

    pair = 2 * M
    lower = before(pair)
    slot = lax.broadcasted_iota(jnp.int32, (2 * cap, pair), 0)
    first_slot = lax.broadcasted_iota(jnp.int32, (2 * cap, pair), 1) // M * cap
    slot = (slot - first_slot).astype(F32)

    @pl.loop(0, G)
    def _(g):
        w_row = w_ref[g]
        m = (w_row > 0.0).astype(F32)
        hit = (slot == rank_of(m, lower)).astype(F32) * m
        sel[g] = hit.astype(BF16)
        w_slot[g] = jnp.broadcast_to(jnp.sum(hit * w_row, axis=1, keepdims=True), w_slot.shape[1:])

    lower = before(M)
    slot = lax.broadcasted_iota(jnp.int32, (cap, M), 0).astype(F32)

    def own_hit(p):
        m = (ct[p] > 0.0).astype(F32)
        return (slot == rank_of(m, lower)).astype(F32) * m

    @pl.loop(0, G)
    def _(g):
        own_sel[g] = jnp.concatenate([own_hit(2 * g), own_hit(2 * g + 1)], axis=0).astype(BF16)

    early = max(0, chunks - DIRECT) if paired else 0
    last = flip(g0, upper)

    def z_copy(i, g):
        return rcopy(zout.at[i, g], zrec.at[i, g0], pz_s.at[0], pz_r.at[i], ep=2 * g + par)

    def z_in(i):
        some = pl.ds(0, upper if i < early else G - 1)
        return rcopy(zout.at[i, some], zrec.at[i, some], pz_s.at[0], pz_r.at[i], ep=mate)

    def z_pair(i):
        some = pl.ds(0, upper - 1)
        rcopy(zout.at[i, some], zpair.at[i, some], pz_s.at[0], zx_r.at[i], ep=mate).wait_recv()
        total = zlast[i]
        for low in range(1, upper):
            total = total + zpair[i, flip(g0, low)].astype(F32)
        zout[i, last] = total.astype(BF16)
        z_copy(i, last).start()

    nb_all = rcopy(xin.at[rest, core], xin.at[rest, core], nf_s.at[0], nf_r.at[0], tp=beside)
    nb_all.wait_recv()
    for i in range(chunks):
        w_in(i).wait_recv()
        z = dot(xin[...].reshape(G * M, 2 * R), wall[i].reshape(2 * R, CW)).reshape(G, M, CW)
        zf[...] = z
        zout[i] = z.astype(BF16)

        if i < early:
            for low in range(1, upper):
                to = flip(g0, low)
                g = flip(to, upper)
                rcopy(zout.at[i, g], zpair.at[i, g0], pz_s.at[0], zx_r.at[i], ep=2 * to + par).start()
                z_copy(i, to).start()
            zlast[i] = zf[last]
        else:
            @pl.loop(1, G)
            def _(k):
                z_copy(i, peer_group(k)).start()

        acc[:, i * CW:(i + 1) * CW] = zf[g0]
        if 0 <= i - 2 < early:
            z_pair(i - 2)

    for i in range(max(0, chunks - 2), early):
        z_pair(i)

    for i in range(chunks):
        z_in(i).wait_recv()

        @pl.loop(0 if i < early else 1, upper if i < early else G)
        def _(k):
            g = flip(g0, k + 1) if i < early else peer_group(k)
            acc[:, i * CW:(i + 1) * CW] += zrec[i, g].astype(F32)

    x_b = acc[:, :C].astype(BF16)
    y_b = acc[:, C:].astype(BF16)
    for i in range(1, conv_old.shape[0]):
        conv_new[i - 1] = conv_old[i]
    conv_new[conv_old.shape[0] - 1] = x_b
    conv_pre = conv_old[0].astype(F32) * taps[0:1, :].astype(F32)
    for i in range(1, taps.shape[0] - 1):
        conv_pre = conv_pre + conv_old[i].astype(F32) * taps[i:i + 1, :].astype(F32)
    conv = (conv_pre + x_b.astype(F32) * taps[taps.shape[0] - 1:, :].astype(F32)).astype(BF16)
    gi, gd = [], []
    for i in range(C // width):
        g = dot(conv[:, i * width:(i + 1) * width], bd[i])
        gi.append(g[:, :width])
        gd.append(g[:, width:])
    gate_in = jax.nn.sigmoid(jnp.concatenate(gi, axis=1))
    gate_dec = jax.nn.sigmoid(jnp.concatenate(gd, axis=1))
    dp = decay_param[...]
    log_decay = decay_scale * gate_dec * (jnp.minimum(dp, 0.0) - jnp.log1p(jnp.exp(-jnp.abs(dp))))
    decay = jnp.exp(log_decay)
    inject = jnp.sqrt(-jnp.tanh(log_decay) * (1.0 + decay * decay))
    state = decay * lru[...] + inject * gate_in * conv.astype(F32)
    new_lru[...] = state
    gated = (state * jax.nn.gelu(y_b.astype(F32), approximate=True)).astype(BF16)

    loads[0].wait()
    order = [tp_peer(k) for k in (2, 3, 1)] if T == 4 else [tp_peer(k) for k in range(1, T)]
    for j in order:
        cols = pl.ds(pl.multiple_of(j * C, 128), C)
        mbuf[j] = dot(gated, po[:, cols]).astype(BF16)
        rcopy(mbuf.at[j], mrec.at[t], mx_s.at[0], mx_r.at[0], tp=j).start()
    mixer = dot(gated, po[:, own_cols]).astype(BF16).astype(F32)
    mx_all = rcopy(mbuf.at[pl.ds(0, T - 1)], mrec.at[pl.ds(0, T - 1)], mx_s.at[0], mx_r.at[0], tp=across)
    mx_all.wait_recv()
    for j in order:
        mixer = mixer + mrec[j].astype(F32)
    summed = (hidden[:, own_cols].astype(F32) + mixer).astype(BF16)
    summed_ref[...] = summed
    sf = summed.astype(F32)
    ssq = jnp.sum(sf * sf, axis=1, keepdims=True)
    same = lax.broadcasted_iota(jnp.int32, (M, M), 0) == lax.broadcasted_iota(jnp.int32, (M, M), 1)
    me = t * E + e
    ssq_row = jnp.sum(jnp.where(same, ssq, 0.0), axis=0, keepdims=True)
    srow[t] = ssq_row
    ssq_all = rcopy(srow.at[pl.ds(0, T - 1)], srow.at[pl.ds(0, T - 1)], q_s.at[0], q_r.at[0], tp=across)
    scale_all = rcopy(stot.at[others], stot.at[others], qe_s.at[0], qe_r.at[0], ep=mate)
    everyone = pl.ds(0, E * T - 1)
    xall[me] = (sf * ffn_gain[own_cols].reshape(1, C).astype(F32)).astype(BF16)

    to_across = core * (across - t)
    to_mate = (1 - core) * (mate - e)
    first = dict(ep=e + to_mate, tp=t + to_across)
    second = dict(ep=e + core * (mate - e), tp=t + (1 - core) * (across - t))

    def slice_a(k):
        return t, 2 * peer_group(k) + par

    def slice_b(k):
        q, s = slice_a(k)
        return q + to_across, s + (1 - core) * (mate_of(s) - s)

    def slice_c(k):
        q, s = slice_a(k)
        return q + (1 - core) * (across - t), s + core * (mate_of(s) - s)

    def slice_d(k):
        q, s = slice_a(k)
        return across, mate_of(s)

    def move(at, r, **to):
        q, s = at
        return rcopy(xall.at[q * E + s], xall.at[q * E + s], x_s.at[0], r, **to)

    def landed(i, k):
        move(slice_a(k), x_r.at[i, peer_group(k)], ep=mate).wait_recv()

    def rail_a(k):
        return move(slice_a(0), x_r.at[0, g0], ep=2 * peer_group(k) + par)

    def rail_b(k):
        return move(slice_b(0), x_r.at[1, g0], ep=2 * peer_group(k) + par)

    def first_a(k):
        return move(slice_a(k), x_r.at[1, peer_group(k)], **first)

    def second_a(k):
        return move(slice_a(k), x_r.at[2, peer_group(k)], **second)

    def second_b(k):
        return move(slice_b(k), x_r.at[3, peer_group(k)], **second)

    def beside_of(i, k):
        return move((slice_a, slice_b, slice_c, slice_d)[i](k), xb_r.at[peer_group(k)], tp=beside)

    def pass_on(i, k):
        if i == 0:
            second_a(k).start()
        if i == 1:
            second_b(k).start()
        beside_of(i, k).start()

    first_a(0).start()

    @pl.loop(1, G)
    def _(k):
        rail_a(k).start()

    pass_on(0, 0)
    for j in order:
        rcopy(srow.at[t], srow.at[t], q_s.at[0], q_r.at[0], tp=j).start()
    own_dw.wait()
    peers = pl.ds(0, T - 1)
    dw_all = rcopy(dwp.at[peers], dwr.at[peers], dw_s.at[0], dw_r.at[0], tp=across)
    dw_all.wait_recv()
    square = (
        lax.broadcasted_iota(jnp.int32, (pair, pair), 0) == lax.broadcasted_iota(jnp.int32, (pair, pair), 1)
    )

    def a_copy(q, g, r, to):
        return rcopy(aall.at[q, g], aall.at[q, g], a_s.at[0], r.at[g], tp=to)

    def pair_in(k):
        g = peer_group(k)
        for i in range(2):
            prow[:, i * M:(i + 1) * M] = stot[2 * g + i]
        rcopy(xall.at[pl.ds(0, 4)], xall.at[pl.ds(0, 4)], x_s.at[0], xb_r.at[g], tp=beside).wait_recv()
        scale_row = lax.rsqrt(prow[...] * (1.0 / D) + epsilon)
        scale = jnp.sum(jnp.where(square, scale_row, 0.0), axis=1, keepdims=True)
        h = None
        for q in range(T):
            part = dot(xall[pl.ds(q * E + 2 * g, 2)].reshape(pair, C), dwr[q])
            h = part if h is None else h + part
        h = h * scale
        half = h.shape[1] // 2
        act = jax.nn.silu(h) * pltpu.roll(h, half, axis=1)
        aall[t, g] = act[:, :half].astype(BF16)
        a_copy(t, g, a_r, across).start()
        a_copy(t, g, ab_r, beside).start()
        pick = sel[g]
        for q in range(T):
            xe[g, :, q * C:(q + 1) * C] = dot(pick, xall[pl.ds(q * E + 2 * g, 2)].reshape(pair, C)).astype(BF16)
        s_slot[g] = jnp.broadcast_to(
            jnp.sum(pick.astype(F32) * scale_row, axis=1, keepdims=True), s_slot.shape[1:]
        )

    def a_forward(k):
        g = peer_group(k)
        a_copy(across, g, a_r, across).wait_recv()
        a_copy(across, g, ab_r, beside).start()

    gate = jax.nn.sigmoid(branch[...])

    def dense(k):
        g = peer_group(k)
        rcopy(aall.at[pl.ds(0, 2), g], aall.at[pl.ds(0, 2), g], a_s.at[0], ab_r.at[g], tp=beside).wait_recv()
        d = dot(aall[0, g], dd[0])
        for q in range(1, T):
            d = d + dot(aall[q, g], dd[q])
        dtmp[...] = (d * gate).reshape(2, M, C)
        om[g] = dtmp[1 - par].astype(BF16)
        rcopy(om.at[g], orm.at[g], om_s.at[0], om_r.at[g], ep=mate).start()
        dacc[g] = dtmp[par]

    def dense_on(k):
        g = peer_group(k)
        rcopy(om.at[g], orm.at[g], om_s.at[0], om_r.at[g], ep=mate).wait_recv()
        total = dacc[g] + orm[g].astype(F32)
        if paired and k == G - 1:
            oz_pair.wait_recv()
            for low in range(1, upper):
                total = total + ozx[flip(g0, low)].astype(F32)
        oz[g] = total.astype(BF16)
        if paired and upper <= k < G - 1:
            to = flip(g0, k - upper + 1)
            rcopy(oz.at[g], ozx.at[g0], oz_s.at[0], ozx_r.at[0], ep=2 * to + par).start()
        elif paired and k == G - 1:
            rcopy(oz.at[g], ozr.at[g0], oz_s.at[0], ozf_r.at[0], ep=2 * g + par).start()
        else:
            rcopy(oz.at[g], ozr.at[g0], oz_s.at[0], oz_r.at[0], ep=2 * g + par).start()

    direct = pl.ds(0, (upper if paired else G) - 1)
    oz_all = rcopy(oz.at[direct], ozr.at[direct], oz_s.at[0], oz_r.at[0], ep=mate)
    if paired:
        oz_pair = rcopy(oz.at[direct], ozx.at[direct], oz_s.at[0], ozx_r.at[0], ep=mate)

    for l in loads[4:5]:
        l.wait()

    def a_in(k):
        landed(0, k)

        @pl.when(core == 0)
        def _():
            first_a(k).start()

        pass_on(0, k)

    landed(1, 0)

    @pl.when(core == 1)
    def _():
        @pl.loop(1, G)
        def _(j):
            rail_b(j).start()

    pass_on(1, 0)
    if G > 1:
        a_in(1)
    ssq_all.wait_recv()
    total = srow[0]
    for q in range(1, T):
        total = total + srow[q]
    stot[e] = total

    @pl.loop(1, E)
    def _(k):
        rcopy(stot.at[e], stot.at[e], qe_s.at[0], qe_r.at[0], ep=ep_peer(k)).start()


    @pl.loop(1, G + 2)
    def _(k):
        @pl.when(k + 1 < G)
        def _():
            a_in(k + 1)

        @pl.when(k <= G)
        def _():
            landed(2, k - 1)
            pass_on(2, k - 1)

        @pl.when(k < G)
        def _():
            landed(1, k)
            pass_on(1, k)

        @pl.when(k <= G)
        def _():
            landed(3, k - 1)
            pass_on(3, k - 1)

        @pl.when(k == 2)
        def _():
            scale_all.wait_recv()

        @pl.when(k >= 2)
        def _():
            pair_in(k - 2)

        @pl.when(k >= 4)
        def _():
            a_forward(k - 4)

        @pl.when(k >= 6)
        def _():
            dense(k - 6)

    loads[1].wait()
    loads[2].wait()
    FH = eg.shape[1]
    nch = 256 if FH % 256 == 0 else FH
    slots = E * cap

    def hidden_units(n):
        cols = slice(n * nch, (n + 1) * nch)
        rows_in = xe[...].reshape(slots, D)
        scale = s_slot[...].reshape(slots, 128)[:, 0:1]
        g = dot(rows_in, eg[:, cols]) * scale
        u = dot(rows_in, eu[:, cols]) * scale
        hid[:, cols] = (jax.nn.silu(g) * u).astype(BF16)

    if G < 2:
        a_forward(0)
    hidden_units(0)
    if G > 3:
        dense(G - 4)
    for n in range(1, FH // nch):
        hidden_units(n)
        if n == 1:
            if G > 1:
                a_forward(G - 2)
            if G > 2:
                dense(G - 3)
    loads[3].wait()

    def down(j):
        return dot(hid[...], ed[:, pl.ds(pl.multiple_of(j * C, 128), C)])

    def e_copy(i):
        return rcopy(ebuf.at[i], erec.at[i], ed_s.at[0], ed_r.at[i], tp=beside)

    def ex_copy(g):
        return rcopy(ex.at[g], exr.at[g], ex_s.at[0], ex_r.at[g], tp=across)

    def eo_copy(s, p):
        return rcopy(eo.at[s], eor.at[p], eo_s.at[0], eo_r.at[0], ep=s)

    def ex_out(k):
        g = peer_group(k)
        ex[g] = (epart[1, g] + erec[1, g].astype(F32)).astype(BF16)
        ex_copy(g).start()

    def ex_in(k):
        g = peer_group(k)
        ex_copy(g).wait_recv()
        red = epart[0, g] + erec[0, g].astype(F32) + exr[g].astype(F32)
        red = red.astype(BF16).astype(F32) * w_slot[g][:, 0:1]
        eo[pl.ds(2 * g, 2)] = red.reshape(2, cap, C).astype(BF16)
        for i in range(2):
            s = 2 * g + i

            @pl.when(s != e)
            def _():
                eo_copy(s, e).start()

    for i, j in ((1, diagonal), (0, beside)):
        ebuf[i] = down(j).reshape(G, 2 * cap, C).astype(BF16)
        e_copy(i).start()
    if G > 1:
        a_forward(G - 1)
        dense(G - 2)
    epart[1] = down(across).reshape(G, 2 * cap, C)
    epart[0] = down(t).reshape(G, 2 * cap, C)
    e_copy(1).wait_recv()

    @pl.loop(0, G)
    def _(k):
        ex_out(G - 1 - k)

    dense(G - 1)
    for k in range(1, G - 1):
        dense_on(k)
    e_copy(0).wait_recv()

    @pl.loop(0, G - 1)
    def _(k):
        ex_in(G - 1 - k)

    if G > 1:
        dense_on(G - 1)
    ex_in(0)
    eor[e] = eo[e]
    rcopy(om.at[g0], orm.at[g0], om_s.at[0], om_r.at[g0], ep=mate).wait_recv()
    acc[:, :C] = summed_ref[...].astype(F32) + dacc[g0] + orm[g0].astype(F32)

    oz_all.wait_recv()
    if paired:
        oz_last = rcopy(oz.at[g0], ozr.at[g0], oz_s.at[0], ozf_r.at[0], ep=mate)
        oz_last.wait_recv()
        for mask in (*range(1, upper), upper):
            acc[:, :C] += ozr[flip(g0, mask)].astype(F32)
    else:
        for k in range(1, G):
            acc[:, :C] += ozr[peer_group(k)].astype(F32)


    eo_all = rcopy(eo.at[others], eor.at[others], eo_s.at[0], eo_r.at[0], ep=mate)
    eo_all.wait_recv()

    picked = eor[...].astype(F32).reshape(slots, C).astype(BF16)
    new_hidden[...] = (
        acc[:, :C] + lax.dot_general(
            own_sel[...].reshape(slots, M), picked, (((0,), (0,)), ((), ())), preferred_element_type=F32
        )
    ).astype(BF16)
    for copy in (ct_all, nb_all, dw_all, mx_all, ssq_all, scale_all, eo_all):
        copy.wait_send()
    z_all = zout.at[:, rest]
    for ref, sem in (
        (wall.at[:, par], w_s), (nb.at[rest, core], nb_s), (z_all, pz_s), (xall.at[everyone], x_s),
        (aall.at[pl.ds(0, 3)], a_s), (ebuf, ed_s), (ex, ex_s), (om, om_s), (oz.at[rest], oz_s),
    ):
        rcopy(ref, ref, sem.at[0], sem.at[0], tp=across).wait_send()


def store_kernel(a, b, c, a_out, b_out, c_out, sems):
    copies = [
        pltpu.make_async_copy(src, dst, sems.at[i])
        for i, (src, dst) in enumerate(((a, a_out), (b, b_out), (c, c_out)))
    ]
    for copy in copies:
        copy.start()
    for copy in copies:
        copy.wait()


def on_device(
    hidden, mix_gain, proj_x, proj_y, conv_taps, input_gate, decay_gate, decay_param,
    proj_out, conv_state, lru_state, ffn_gain, routes, route_weights,
    expert_gate, expert_up, expert_down, dense_gate, dense_up, dense_down, branch_gate,
):
    E = lax.axis_size("ep")
    T = lax.axis_size("tp")
    M, D = hidden.shape
    C = D // T
    R = proj_x.shape[0]
    N = E * M
    heads, block = input_gate.shape[:2]
    group = max(1, 128 // block)

    experts = expert_gate.shape[0] * E
    cap = -(-(M * routes.shape[1] // experts + 2) // 8) * 8
    slots = E * cap
    G = E // 2
    h = dense_gate.shape[1] // T
    half = -(-2 * h // 128) * 64

    dd = jnp.pad(dense_down.reshape(T, h, C), ((0, 0), (0, half - h), (0, 0)))
    FH = expert_gate.shape[2]
    vm = pl.BlockSpec(memory_space=pltpu.VMEM)
    anyspace = pl.BlockSpec(memory_space=pl.ANY)
    DMA = pltpu.SemaphoreType.DMA
    V = pltpu.VMEM
    chunks = max(1, 2 * C // 128)
    small = (
        hidden, mix_gain, routes.T, route_weights.T, conv_state.transpose(1, 0, 2), conv_taps,
        input_gate, decay_gate, decay_param[None, :], lru_state,
        ffn_gain, branch_gate[None, :],
    )
    scratch = [
        *(V(a.shape, a.dtype) for a in small),
        V((E, 1, M), F32), V((G, 1, 2 * M), F32), V((heads // group, group * block, 2 * group * block), BF16),
        V((chunks, 2, R, 2 * C // chunks), BF16), V((C, T * h), BF16), V((C, T * h), BF16),
        V((C, D), BF16), V((D, FH), BF16), V((D, FH), BF16), V((FH, D), BF16), V((T, half, C), BF16),
        V((G, 2, M // 2, 2 * R), BF16), V((T, C, 2 * half), BF16), V((T, C, 2 * half), BF16),
        V((G, 2, M // 2, 2 * R), BF16), V((G, M, 2 * C // chunks), F32), V((chunks, M, 2 * C // chunks), F32),
        V((chunks, G, M, 2 * C // chunks), BF16),
        V((chunks, G, M, 2 * C // chunks), BF16), V((chunks, G, M, 2 * C // chunks), BF16),
        V((E, 1, M), F32), V((M, 2 * C), F32),
        V((T, M, C), BF16), V((T, M, C), BF16), V((T, 1, M), F32), V((E, 1, M), F32), V((1, 2 * M), F32),
        V((T * E, M, C), BF16), V((T, G, 2 * M, half), BF16),
        V((G, 2 * cap, D), BF16), V((slots, FH), BF16), V((G, 2 * cap, 2 * M), BF16),
        V((G, 2 * cap, M), BF16), V((G, 2 * cap, 128), F32), V((G, 2 * cap, 128), F32),
        V((2, G, 2 * cap, C), BF16), V((2, G, 2 * cap, C), BF16), V((2, G, 2 * cap, C), F32),
        V((G, 2 * cap, C), BF16), V((G, 2 * cap, C), BF16), V((E, cap, C), BF16), V((E, cap, C), BF16),
        V((2, M, C), F32),
        V((G, M, C), BF16), V((G, M, C), F32), V((G, M, C), BF16), V((G, M, C), BF16), V((G, M, C), BF16),
        V((G, M, C), BF16), V((M, C), BF16),
        DMA((8,)), DMA((12,)), DMA((1,)), DMA((1,)), DMA((chunks,)),
        DMA((1,)), DMA((G,)), DMA((1,)), DMA((1,)), DMA((1,)), DMA((1,)), DMA((1,)), DMA((chunks,)), DMA((chunks,)),
        DMA((1,)), DMA((1,)), DMA((1,)), DMA((1,)), DMA((1,)), DMA((1,)), DMA((1,)), DMA((1,)),
        DMA((1,)), DMA((4, G)), DMA((G,)), DMA((1,)), DMA((G,)), DMA((G,)),
        DMA((1,)), DMA((2,)), DMA((1,)), DMA((G,)), DMA((1,)), DMA((1,)),
        DMA((1,)), DMA((G,)), DMA((1,)), DMA((1,)), DMA((1,)), DMA((1,)),
    ]
    outs = pl.pallas_call(
        functools.partial(layer_kernel, E, T, cap),
        out_shape=(V((M, C), BF16), V((M, C), F32), V((conv_state.shape[1], M, C), BF16)),
        in_specs=[anyspace] * 21,
        out_specs=(vm, vm, vm),
        scratch_shapes=scratch,
        compiler_params=pltpu.CompilerParams(
            collective_id=0, has_side_effects=True, vmem_limit_bytes=60 * 1024 * 1024
        ),
    )(
        *small,
        proj_x, proj_y, dense_gate, dense_up, proj_out, expert_gate[0], expert_up[0], expert_down[0], dd,
    )
    new_hidden, new_lru, new_conv = pl.pallas_call(
        store_kernel,
        out_shape=tuple(jax.ShapeDtypeStruct(o.shape, o.dtype) for o in outs),
        in_specs=[vm] * 3,
        out_specs=(anyspace,) * 3,
        scratch_shapes=[DMA((3,))],
    )(*(pltpu.with_memory_space_constraint(o, pltpu.VMEM) for o in outs))
    return (new_hidden, new_lru, new_conv.transpose(1, 0, 2))


def solution(mesh):
    in_specs = (
        P("ep", None),
        P(),
        P("ep", "tp"),
        P("ep", "tp"),
        P(None, "tp"),
        P("tp", None, None),
        P("tp", None, None),
        P("tp"),
        P("tp", None),
        P("ep", None, "tp"),
        P("ep", "tp"),
        P(),
        P("ep", None),
        P("ep", None),
        P("ep", None, "tp"),
        P("ep", None, "tp"),
        P("ep", "tp", None),
        P("tp", "ep"),
        P("tp", "ep"),
        P("ep", "tp"),
        P("tp"),
    )
    out_specs = (P("ep", "tp"), P("ep", "tp"), P("ep", None, "tp"))
    return jax.shard_map(
        on_device, mesh=mesh, in_specs=in_specs, out_specs=out_specs, check_vma=False
    )
```

```python
import functools

import jax
import jax.numpy as jnp
from jax import lax
from jax.experimental import pallas as pl
from jax.experimental.pallas import tpu as pltpu
from jax.sharding import PartitionSpec as P

epsilon = 1e-06
decay_scale = 8.0
MESH = pl.DeviceIdType.MESH
DIRECT = 3
F32 = jnp.float32
BF16 = jnp.bfloat16


def dot(a, b):
    return jnp.dot(a, b, preferred_element_type=F32)


def layer_kernel(
    E, T, cap,
    hidden_h, mix_gain_h, routes_h, weights_h, conv_old_h, taps_h, ig_h, dgate_h, decay_param_h, lru_h,
    ffn_gain_h, branch_h,
    wx_h, wy_h, dg_h, du_h, po_h, eg_h, eu_h, ed_h, dd_h,
    new_hidden, new_lru, conv_new,
    hidden, mix_gain, routes, weights, conv_old, taps, ig, dgate, decay_param, lru, ffn_gain, branch,
    ct, w_ref, bd, wall, dg, du, po, eg, eu, ed, dd, nb, dwp, dwr, xin, zf, zlast, zpair, zout, zrec, ctr, acc,
    mbuf, mrec, srow, stot, prow, xall, aall, xe, hid, sel, own_sel, w_slot, s_slot,
    ebuf, erec, epart, ex, exr, eo, eor, dtmp, om, dacc, orm, oz, ozr, ozx, summed_ref,
    load_sem, in_l, w_l, w_s, w_r, nb_s, nb_r, nf_s, nf_r, ct_s, ct_r, pz_s, pz_r, zx_r, dw_s, dw_r, mx_s, mx_r, q_s, q_r, qe_s, qe_r,
    x_s, x_r, xb_r, a_s, a_r, ab_r, ed_s, ed_r, ex_s, ex_r, eo_s, eo_r, om_s, om_r, oz_s, oz_r, ozx_r, ozf_r,
):
    e = lax.axis_index("ep")
    t = lax.axis_index("tp")
    M, D = hidden.shape
    C = D // T
    R = wx_h.shape[0]
    chunks, CW = wall.shape[0], wall.shape[3]
    G = E // 2
    g0 = e // 2
    par = lax.rem(e, 2)
    mate = e + 1 - 2 * par
    own_cols = pl.ds(pl.multiple_of(t * C, 128), C)

    def ep_peer(k):
        return lax.rem(e + k, E)

    def ep_from(k):
        return lax.rem(e + E - k, E)

    def group(k):
        return lax.rem(g0 + k, G)

    def rail_from(k):
        return 2 * lax.rem(g0 + G - k, G) + par

    def mate_of(s):
        return s + 1 - 2 * lax.rem(s, 2)

    upper = G // 2
    paired = G > 2 and G & (G - 1) == 0

    def flip(g, mask):
        out, bit = 0, 1
        while bit < G:
            out = out + bit * lax.rem(g // bit + mask // bit, 2)
            bit *= 2
        return out

    def peer_group(k):
        if not paired:
            return lax.rem(g0 + k, G)
        return flip(g0, k // upper * upper + lax.rem(k + k // upper, upper))

    def tp_peer(k):
        return lax.rem(t + k, T)

    across = lax.rem(t + T // 2, T)
    beside = t + 1 - 2 * lax.rem(t, 2)
    diagonal = lax.rem(beside + T // 2, T)

    inputs = [
        pltpu.make_async_copy(src, dst, in_l.at[i])
        for i, (src, dst) in enumerate(
            ((hidden_h, hidden), (mix_gain_h, mix_gain), (routes_h, routes), (weights_h, weights),
             (conv_old_h, conv_old), (taps_h, taps), (ig_h, ig), (dgate_h, dgate),
             (decay_param_h, decay_param), (lru_h, lru), (ffn_gain_h, ffn_gain), (branch_h, branch))
        )
    ]
    for copy in inputs[:4]:
        copy.start()

    barrier = pltpu.get_barrier_semaphore()

    @pl.loop(1, E)
    def _(k):
        pl.semaphore_signal(barrier, inc=1, device_id=(ep_peer(k), t), device_id_type=MESH)

    for k in range(1, T):
        pl.semaphore_signal(barrier, inc=1, device_id=(e, tp_peer(k)), device_id_type=MESH)

    loads = [
        pltpu.make_async_copy(src, dst, load_sem.at[i])
        for i, (src, dst) in enumerate(
            ((po_h, po), (eg_h, eg), (eu_h, eu), (ed_h, ed), (dd_h, dd),
             (dg_h, dg), (du_h, du))
        )
    ]
    own_dw = pltpu.make_async_copy(dwp.at[t], dwr.at[t], load_sem.at[7])

    def w_load(i):
        src, col = (wx_h, i * CW) if i * CW < C else (wy_h, i * CW - C)
        return pltpu.make_async_copy(src.at[:, pl.ds(col, CW)], wall.at[i, par], w_l.at[0])

    for i in range(chunks):
        w_load(i).start()
    for i in (5, 6, 0):
        loads[i].start()
    for copy in inputs[4:]:
        copy.start()

    def rcopy(src, dst, s, r, ep=None, tp=None):
        return pltpu.make_async_remote_copy(
            src_ref=src, dst_ref=dst, send_sem=s, recv_sem=r,
            device_id=(e if ep is None else ep, t if tp is None else tp),
            device_id_type=MESH,
        )

    for copy in inputs[:4]:
        copy.wait()
    hf = hidden[...].astype(F32)
    inv = lax.rsqrt(jnp.mean(hf * hf, axis=-1, keepdims=True) + epsilon)
    normed = (hf * inv * mix_gain[...].reshape(1, D).astype(F32)).astype(BF16)
    for g in range(G):
        nb[g] = normed[:, 2 * g * R:2 * (g + 1) * R].reshape(2, M // 2, 2 * R)
    for p in range(E):
        ct[p] = jnp.sum(jnp.where(routes[...] == p, weights[...], 0.0), axis=0, keepdims=True)
    pl.semaphore_wait(barrier, E - 1 + T - 1)

    core = lax.rem(t, 2)

    def w_copy(i):
        return rcopy(wall.at[i, par], wall.at[i, par], w_s.at[0], w_r.at[i], ep=mate)

    def w_in(i):
        return rcopy(wall.at[i, 1 - par], wall.at[i, 1 - par], w_s.at[0], w_r.at[i], ep=mate)

    def nb_copy(g):
        return rcopy(nb.at[g, core], xin.at[g0, core], nb_s.at[0], nb_r.at[g0], ep=2 * g + par)

    def nb_in(g):
        return rcopy(nb.at[g, core], xin.at[g, core], nb_s.at[0], nb_r.at[g], ep=mate)

    def nb_beside(g):
        return rcopy(xin.at[g, core], xin.at[g, core], nf_s.at[0], nf_r.at[0], tp=beside)

    rest = pl.ds(0, G - 1)

    @pl.loop(1, E)
    def _(k):
        p = ep_peer(k)
        rcopy(ct.at[p], ctr.at[e], ct_s.at[0], ct_r.at[0], ep=p).start()

    @pl.loop(1, G)
    def _(k):
        nb_copy(peer_group(k)).start()

    pltpu.make_async_copy(wall.at[:, par], wall.at[:, par], w_l.at[0]).wait()
    for i in range(chunks):
        w_copy(i).start()

    loads[5].wait()
    loads[6].wait()
    h = dg.shape[1] // T
    half = dwp.shape[2] // 2
    if half != h:
        dwp[...] = jnp.zeros_like(dwp)
    for j in range(T):
        dwp[j, :, :h] = dg[:, j * h:(j + 1) * h]
        dwp[j, :, half:half + h] = du[:, j * h:(j + 1) * h]
    own_dw.start()
    for k in range(1, T):
        j = tp_peer(k)
        rcopy(dwp.at[j], dwr.at[t], dw_s.at[0], dw_r.at[0], tp=j).start()
    for l in loads[1:5]:
        l.start()

    for copy in inputs[4:]:
        copy.wait()
    xin[g0] = nb[g0]

    @pl.loop(1, G)
    def _(k):
        g = peer_group(k)
        nb_in(g).wait_recv()
        nb_beside(g).start()

    early = max(0, chunks - DIRECT) if paired else 0
    last = flip(g0, upper)

    def z_copy(i, g):
        return rcopy(zout.at[i, g], zrec.at[i, g0], pz_s.at[0], pz_r.at[i], ep=2 * g + par)

    def z_in(i):
        some = pl.ds(0, upper if i < early else G - 1)
        return rcopy(zout.at[i, some], zrec.at[i, some], pz_s.at[0], pz_r.at[i], ep=mate)

    def z_pair(i):
        some = pl.ds(0, upper - 1)
        rcopy(zout.at[i, some], zpair.at[i, some], pz_s.at[0], zx_r.at[i], ep=mate).wait_recv()
        total = zlast[i]
        for low in range(1, upper):
            total = total + zpair[i, flip(g0, low)].astype(F32)
        zout[i, last] = total.astype(BF16)
        z_copy(i, last).start()

    nb_all = rcopy(xin.at[rest, core], xin.at[rest, core], nf_s.at[0], nf_r.at[0], tp=beside)
    nb_all.wait_recv()
    for i in range(chunks):
        w_in(i).wait_recv()
        z = dot(xin[...].reshape(G * M, 2 * R), wall[i].reshape(2 * R, CW)).reshape(G, M, CW)
        zf[...] = z
        zout[i] = z.astype(BF16)

        if i < early:
            for low in range(1, upper):
                to = flip(g0, low)
                g = flip(to, upper)
                rcopy(zout.at[i, g], zpair.at[i, g0], pz_s.at[0], zx_r.at[i], ep=2 * to + par).start()
                z_copy(i, to).start()
            zlast[i] = zf[last]
        else:
            @pl.loop(1, G)
            def _(k):
                z_copy(i, peer_group(k)).start()

        acc[:, i * CW:(i + 1) * CW] = zf[g0]
        if 0 <= i - 2 < early:
            z_pair(i - 2)

    for i in range(max(0, chunks - 2), early):
        z_pair(i)

    others = pl.ds(0, E - 1)
    ct_all = rcopy(ct.at[others], ctr.at[others], ct_s.at[0], ct_r.at[0], ep=mate)
    ct_all.wait_recv()

    ctr[e] = ct[e]
    for s in range(E):
        w_ref[s // 2, :, s % 2 * M:(s % 2 + 1) * M] = ctr[s]
    bd[...] = jnp.zeros_like(bd)
    block = ig.shape[1]
    width = bd.shape[1]
    per = width // block
    for i in range(ig.shape[0]):
        lo = i % per * block
        bd[i // per, lo:lo + block, lo:lo + block] = ig[i]
        bd[i // per, lo:lo + block, width + lo:width + lo + block] = dgate[i]
    def before(n):
        row = lax.broadcasted_iota(jnp.int32, (n, n), 0)
        col = lax.broadcasted_iota(jnp.int32, (n, n), 1)
        return ((row < col) & (row // M == col // M)).astype(F32).astype(BF16)

    def rank_of(m, earlier):
        rows = max(16, m.shape[0])
        return dot(jnp.broadcast_to(m, (rows, m.shape[1])).astype(BF16), earlier)[0:1]

    pair = 2 * M
    lower = before(pair)
    slot = lax.broadcasted_iota(jnp.int32, (2 * cap, pair), 0)
    first_slot = lax.broadcasted_iota(jnp.int32, (2 * cap, pair), 1) // M * cap
    slot = (slot - first_slot).astype(F32)

    @pl.loop(0, G)
    def _(g):
        w_row = w_ref[g]
        m = (w_row > 0.0).astype(F32)
        hit = (slot == rank_of(m, lower)).astype(F32) * m
        sel[g] = hit.astype(BF16)
        w_slot[g] = jnp.broadcast_to(jnp.sum(hit * w_row, axis=1, keepdims=True), w_slot.shape[1:])

    lower = before(M)
    slot = lax.broadcasted_iota(jnp.int32, (cap, M), 0).astype(F32)

    def own_hit(p):
        m = (ct[p] > 0.0).astype(F32)
        return (slot == rank_of(m, lower)).astype(F32) * m

    @pl.loop(0, G)
    def _(g):
        own_sel[g] = jnp.concatenate([own_hit(2 * g), own_hit(2 * g + 1)], axis=0).astype(BF16)

    for i in range(chunks):
        z_in(i).wait_recv()

        @pl.loop(0 if i < early else 1, upper if i < early else G)
        def _(k):
            g = flip(g0, k + 1) if i < early else peer_group(k)
            acc[:, i * CW:(i + 1) * CW] += zrec[i, g].astype(F32)

    x_b = acc[:, :C].astype(BF16)
    y_b = acc[:, C:].astype(BF16)
    for i in range(1, conv_old.shape[0]):
        conv_new[i - 1] = conv_old[i]
    conv_new[conv_old.shape[0] - 1] = x_b
    conv_pre = conv_old[0].astype(F32) * taps[0:1, :].astype(F32)
    for i in range(1, taps.shape[0] - 1):
        conv_pre = conv_pre + conv_old[i].astype(F32) * taps[i:i + 1, :].astype(F32)
    conv = (conv_pre + x_b.astype(F32) * taps[taps.shape[0] - 1:, :].astype(F32)).astype(BF16)
    gi, gd = [], []
    for i in range(C // width):
        g = dot(conv[:, i * width:(i + 1) * width], bd[i])
        gi.append(g[:, :width])
        gd.append(g[:, width:])
    gate_in = jax.nn.sigmoid(jnp.concatenate(gi, axis=1))
    gate_dec = jax.nn.sigmoid(jnp.concatenate(gd, axis=1))
    dp = decay_param[...]
    log_decay = decay_scale * gate_dec * (jnp.minimum(dp, 0.0) - jnp.log1p(jnp.exp(-jnp.abs(dp))))
    decay = jnp.exp(log_decay)
    inject = jnp.sqrt(-jnp.tanh(log_decay) * (1.0 + decay * decay))
    state = decay * lru[...] + inject * gate_in * conv.astype(F32)
    new_lru[...] = state
    gated = (state * jax.nn.gelu(y_b.astype(F32), approximate=True)).astype(BF16)

    loads[0].wait()
    order = [tp_peer(k) for k in (2, 3, 1)] if T == 4 else [tp_peer(k) for k in range(1, T)]
    for j in order:
        cols = pl.ds(pl.multiple_of(j * C, 128), C)
        mbuf[j] = dot(gated, po[:, cols]).astype(BF16)
        rcopy(mbuf.at[j], mrec.at[t], mx_s.at[0], mx_r.at[0], tp=j).start()
    mixer = dot(gated, po[:, own_cols]).astype(BF16).astype(F32)
    mx_all = rcopy(mbuf.at[pl.ds(0, T - 1)], mrec.at[pl.ds(0, T - 1)], mx_s.at[0], mx_r.at[0], tp=across)
    mx_all.wait_recv()
    for j in order:
        mixer = mixer + mrec[j].astype(F32)
    summed = (hidden[:, own_cols].astype(F32) + mixer).astype(BF16)
    summed_ref[...] = summed
    sf = summed.astype(F32)
    ssq = jnp.sum(sf * sf, axis=1, keepdims=True)
    same = lax.broadcasted_iota(jnp.int32, (M, M), 0) == lax.broadcasted_iota(jnp.int32, (M, M), 1)
    me = t * E + e
    ssq_row = jnp.sum(jnp.where(same, ssq, 0.0), axis=0, keepdims=True)
    srow[t] = ssq_row
    ssq_all = rcopy(srow.at[pl.ds(0, T - 1)], srow.at[pl.ds(0, T - 1)], q_s.at[0], q_r.at[0], tp=across)
    scale_all = rcopy(stot.at[others], stot.at[others], qe_s.at[0], qe_r.at[0], ep=mate)
    everyone = pl.ds(0, E * T - 1)
    xall[me] = (sf * ffn_gain[own_cols].reshape(1, C).astype(F32)).astype(BF16)

    to_across = core * (across - t)
    to_mate = (1 - core) * (mate - e)
    first = dict(ep=e + to_mate, tp=t + to_across)
    second = dict(ep=e + core * (mate - e), tp=t + (1 - core) * (across - t))

    def slice_a(k):
        return t, 2 * peer_group(k) + par

    def slice_b(k):
        q, s = slice_a(k)
        return q + to_across, s + (1 - core) * (mate_of(s) - s)

    def slice_c(k):
        q, s = slice_a(k)
        return q + (1 - core) * (across - t), s + core * (mate_of(s) - s)

    def slice_d(k):
        q, s = slice_a(k)
        return across, mate_of(s)

    def move(at, r, **to):
        q, s = at
        return rcopy(xall.at[q * E + s], xall.at[q * E + s], x_s.at[0], r, **to)

    def landed(i, k):
        move(slice_a(k), x_r.at[i, peer_group(k)], ep=mate).wait_recv()

    def rail_a(k):
        return move(slice_a(0), x_r.at[0, g0], ep=2 * peer_group(k) + par)

    def rail_b(k):
        return move(slice_b(0), x_r.at[1, g0], ep=2 * peer_group(k) + par)

    def first_a(k):
        return move(slice_a(k), x_r.at[1, peer_group(k)], **first)

    def second_a(k):
        return move(slice_a(k), x_r.at[2, peer_group(k)], **second)

    def second_b(k):
        return move(slice_b(k), x_r.at[3, peer_group(k)], **second)

    def beside_of(i, k):
        return move((slice_a, slice_b, slice_c, slice_d)[i](k), xb_r.at[peer_group(k)], tp=beside)

    def pass_on(i, k):
        if i == 0:
            second_a(k).start()
        if i == 1:
            second_b(k).start()
        beside_of(i, k).start()

    first_a(0).start()

    @pl.loop(1, G)
    def _(k):
        rail_a(k).start()

    pass_on(0, 0)
    for j in order:
        rcopy(srow.at[t], srow.at[t], q_s.at[0], q_r.at[0], tp=j).start()
    own_dw.wait()
    peers = pl.ds(0, T - 1)
    dw_all = rcopy(dwp.at[peers], dwr.at[peers], dw_s.at[0], dw_r.at[0], tp=across)
    dw_all.wait_recv()
    square = (
        lax.broadcasted_iota(jnp.int32, (pair, pair), 0) == lax.broadcasted_iota(jnp.int32, (pair, pair), 1)
    )

    def a_copy(q, g, r, to):
        return rcopy(aall.at[q, g], aall.at[q, g], a_s.at[0], r.at[g], tp=to)

    def pair_in(k):
        g = peer_group(k)
        for i in range(2):
            prow[:, i * M:(i + 1) * M] = stot[2 * g + i]
        rcopy(xall.at[pl.ds(0, 4)], xall.at[pl.ds(0, 4)], x_s.at[0], xb_r.at[g], tp=beside).wait_recv()
        scale_row = lax.rsqrt(prow[...] * (1.0 / D) + epsilon)
        scale = jnp.sum(jnp.where(square, scale_row, 0.0), axis=1, keepdims=True)
        h = None
        for q in range(T):
            part = dot(xall[pl.ds(q * E + 2 * g, 2)].reshape(pair, C), dwr[q])
            h = part if h is None else h + part
        h = h * scale
        half = h.shape[1] // 2
        act = jax.nn.silu(h) * pltpu.roll(h, half, axis=1)
        aall[t, g] = act[:, :half].astype(BF16)
        a_copy(t, g, a_r, across).start()
        a_copy(t, g, ab_r, beside).start()
        pick = sel[g]
        for q in range(T):
            xe[g, :, q * C:(q + 1) * C] = dot(pick, xall[pl.ds(q * E + 2 * g, 2)].reshape(pair, C)).astype(BF16)
        s_slot[g] = jnp.broadcast_to(
            jnp.sum(pick.astype(F32) * scale_row, axis=1, keepdims=True), s_slot.shape[1:]
        )

    def a_forward(k):
        g = peer_group(k)
        a_copy(across, g, a_r, across).wait_recv()
        a_copy(across, g, ab_r, beside).start()

    gate = jax.nn.sigmoid(branch[...])

    def dense(k):
        g = peer_group(k)
        rcopy(aall.at[pl.ds(0, 2), g], aall.at[pl.ds(0, 2), g], a_s.at[0], ab_r.at[g], tp=beside).wait_recv()
        d = dot(aall[0, g], dd[0])
        for q in range(1, T):
            d = d + dot(aall[q, g], dd[q])
        dtmp[...] = (d * gate).reshape(2, M, C)
        om[g] = dtmp[1 - par].astype(BF16)
        rcopy(om.at[g], orm.at[g], om_s.at[0], om_r.at[g], ep=mate).start()
        dacc[g] = dtmp[par]

    def dense_on(k):
        g = peer_group(k)
        rcopy(om.at[g], orm.at[g], om_s.at[0], om_r.at[g], ep=mate).wait_recv()
        total = dacc[g] + orm[g].astype(F32)
        if paired and k == G - 1:
            oz_pair.wait_recv()
            for low in range(1, upper):
                total = total + ozx[flip(g0, low)].astype(F32)
        oz[g] = total.astype(BF16)
        if paired and upper <= k < G - 1:
            to = flip(g0, k - upper + 1)
            rcopy(oz.at[g], ozx.at[g0], oz_s.at[0], ozx_r.at[0], ep=2 * to + par).start()
        elif paired and k == G - 1:
            rcopy(oz.at[g], ozr.at[g0], oz_s.at[0], ozf_r.at[0], ep=2 * g + par).start()
        else:
            rcopy(oz.at[g], ozr.at[g0], oz_s.at[0], oz_r.at[0], ep=2 * g + par).start()

    direct = pl.ds(0, (upper if paired else G) - 1)
    oz_all = rcopy(oz.at[direct], ozr.at[direct], oz_s.at[0], oz_r.at[0], ep=mate)
    if paired:
        oz_pair = rcopy(oz.at[direct], ozx.at[direct], oz_s.at[0], ozx_r.at[0], ep=mate)

    for l in loads[4:5]:
        l.wait()

    def a_in(k):
        landed(0, k)

        @pl.when(core == 0)
        def _():
            first_a(k).start()

        pass_on(0, k)

    landed(1, 0)

    @pl.when(core == 1)
    def _():
        @pl.loop(1, G)
        def _(j):
            rail_b(j).start()

    pass_on(1, 0)
    if G > 1:
        a_in(1)
    ssq_all.wait_recv()
    total = srow[0]
    for q in range(1, T):
        total = total + srow[q]
    stot[e] = total

    @pl.loop(1, E)
    def _(k):
        rcopy(stot.at[e], stot.at[e], qe_s.at[0], qe_r.at[0], ep=ep_peer(k)).start()


    @pl.loop(1, G + 2)
    def _(k):
        @pl.when(k + 1 < G)
        def _():
            a_in(k + 1)

        @pl.when(k <= G)
        def _():
            landed(2, k - 1)
            pass_on(2, k - 1)

        @pl.when(k < G)
        def _():
            landed(1, k)
            pass_on(1, k)

        @pl.when(k <= G)
        def _():
            landed(3, k - 1)
            pass_on(3, k - 1)

        @pl.when(k == 2)
        def _():
            scale_all.wait_recv()

        @pl.when(k >= 2)
        def _():
            pair_in(k - 2)

        @pl.when(k >= 4)
        def _():
            a_forward(k - 4)

        @pl.when(k >= 6)
        def _():
            dense(k - 6)

    loads[1].wait()
    loads[2].wait()
    FH = eg.shape[1]
    nch = 256 if FH % 256 == 0 else FH
    slots = E * cap

    def hidden_units(n):
        cols = slice(n * nch, (n + 1) * nch)
        rows_in = xe[...].reshape(slots, D)
        scale = s_slot[...].reshape(slots, 128)[:, 0:1]
        g = dot(rows_in, eg[:, cols]) * scale
        u = dot(rows_in, eu[:, cols]) * scale
        hid[:, cols] = (jax.nn.silu(g) * u).astype(BF16)

    if G < 2:
        a_forward(0)
    hidden_units(0)
    if G > 3:
        dense(G - 4)
    for n in range(1, FH // nch):
        hidden_units(n)
        if n == 1:
            if G > 1:
                a_forward(G - 2)
            if G > 2:
                dense(G - 3)
    loads[3].wait()

    def down(j):
        return dot(hid[...], ed[:, pl.ds(pl.multiple_of(j * C, 128), C)])

    def e_copy(i):
        return rcopy(ebuf.at[i], erec.at[i], ed_s.at[0], ed_r.at[i], tp=beside)

    def ex_copy(g):
        return rcopy(ex.at[g], exr.at[g], ex_s.at[0], ex_r.at[g], tp=across)

    def eo_copy(s, p):
        return rcopy(eo.at[s], eor.at[p], eo_s.at[0], eo_r.at[0], ep=s)

    def ex_out(k):
        g = peer_group(k)
        ex[g] = (epart[1, g] + erec[1, g].astype(F32)).astype(BF16)
        ex_copy(g).start()

    def ex_in(k):
        g = peer_group(k)
        ex_copy(g).wait_recv()
        red = epart[0, g] + erec[0, g].astype(F32) + exr[g].astype(F32)
        red = red.astype(BF16).astype(F32) * w_slot[g][:, 0:1]
        eo[pl.ds(2 * g, 2)] = red.reshape(2, cap, C).astype(BF16)
        for i in range(2):
            s = 2 * g + i

            @pl.when(s != e)
            def _():
                eo_copy(s, e).start()

    for i, j in ((1, diagonal), (0, beside)):
        ebuf[i] = down(j).reshape(G, 2 * cap, C).astype(BF16)
        e_copy(i).start()
    if G > 1:
        a_forward(G - 1)
        dense(G - 2)
    epart[1] = down(across).reshape(G, 2 * cap, C)
    epart[0] = down(t).reshape(G, 2 * cap, C)
    e_copy(1).wait_recv()

    @pl.loop(0, G)
    def _(k):
        ex_out(G - 1 - k)

    dense(G - 1)
    for k in range(1, G - 1):
        dense_on(k)
    e_copy(0).wait_recv()

    @pl.loop(0, G - 1)
    def _(k):
        ex_in(G - 1 - k)

    if G > 1:
        dense_on(G - 1)
    ex_in(0)
    eor[e] = eo[e]
    rcopy(om.at[g0], orm.at[g0], om_s.at[0], om_r.at[g0], ep=mate).wait_recv()
    acc[:, :C] = summed_ref[...].astype(F32) + dacc[g0] + orm[g0].astype(F32)

    oz_all.wait_recv()
    if paired:
        oz_last = rcopy(oz.at[g0], ozr.at[g0], oz_s.at[0], ozf_r.at[0], ep=mate)
        oz_last.wait_recv()
        for mask in (*range(1, upper), upper):
            acc[:, :C] += ozr[flip(g0, mask)].astype(F32)
    else:
        for k in range(1, G):
            acc[:, :C] += ozr[peer_group(k)].astype(F32)


    eo_all = rcopy(eo.at[others], eor.at[others], eo_s.at[0], eo_r.at[0], ep=mate)
    eo_all.wait_recv()

    picked = eor[...].astype(F32).reshape(slots, C).astype(BF16)
    new_hidden[...] = (
        acc[:, :C] + lax.dot_general(
            own_sel[...].reshape(slots, M), picked, (((0,), (0,)), ((), ())), preferred_element_type=F32
        )
    ).astype(BF16)
    for copy in (ct_all, nb_all, dw_all, mx_all, ssq_all, scale_all, eo_all):
        copy.wait_send()
    z_all = zout.at[:, rest]
    for ref, sem in (
        (wall.at[:, par], w_s), (nb.at[rest, core], nb_s), (z_all, pz_s), (xall.at[everyone], x_s),
        (aall.at[pl.ds(0, 3)], a_s), (ebuf, ed_s), (ex, ex_s), (om, om_s), (oz.at[rest], oz_s),
    ):
        rcopy(ref, ref, sem.at[0], sem.at[0], tp=across).wait_send()


def store_kernel(a, b, c, a_out, b_out, c_out, sems):
    copies = [
        pltpu.make_async_copy(src, dst, sems.at[i])
        for i, (src, dst) in enumerate(((a, a_out), (b, b_out), (c, c_out)))
    ]
    for copy in copies:
        copy.start()
    for copy in copies:
        copy.wait()


def on_device(
    hidden, mix_gain, proj_x, proj_y, conv_taps, input_gate, decay_gate, decay_param,
    proj_out, conv_state, lru_state, ffn_gain, routes, route_weights,
    expert_gate, expert_up, expert_down, dense_gate, dense_up, dense_down, branch_gate,
):
    E = lax.axis_size("ep")
    T = lax.axis_size("tp")
    M, D = hidden.shape
    C = D // T
    R = proj_x.shape[0]
    N = E * M
    heads, block = input_gate.shape[:2]
    group = max(1, 128 // block)

    experts = expert_gate.shape[0] * E
    cap = -(-(M * routes.shape[1] // experts + 2) // 8) * 8
    slots = E * cap
    G = E // 2
    h = dense_gate.shape[1] // T
    half = -(-2 * h // 128) * 64

    dd = jnp.pad(dense_down.reshape(T, h, C), ((0, 0), (0, half - h), (0, 0)))
    FH = expert_gate.shape[2]
    vm = pl.BlockSpec(memory_space=pltpu.VMEM)
    anyspace = pl.BlockSpec(memory_space=pl.ANY)
    DMA = pltpu.SemaphoreType.DMA
    V = pltpu.VMEM
    chunks = max(1, 2 * C // 128)
    small = (
        hidden, mix_gain, routes.T, route_weights.T, conv_state.transpose(1, 0, 2), conv_taps,
        input_gate, decay_gate, decay_param[None, :], lru_state,
        ffn_gain, branch_gate[None, :],
    )
    scratch = [
        *(V(a.shape, a.dtype) for a in small),
        V((E, 1, M), F32), V((G, 1, 2 * M), F32), V((heads // group, group * block, 2 * group * block), BF16),
        V((chunks, 2, R, 2 * C // chunks), BF16), V((C, T * h), BF16), V((C, T * h), BF16),
        V((C, D), BF16), V((D, FH), BF16), V((D, FH), BF16), V((FH, D), BF16), V((T, half, C), BF16),
        V((G, 2, M // 2, 2 * R), BF16), V((T, C, 2 * half), BF16), V((T, C, 2 * half), BF16),
        V((G, 2, M // 2, 2 * R), BF16), V((G, M, 2 * C // chunks), F32), V((chunks, M, 2 * C // chunks), F32),
        V((chunks, G, M, 2 * C // chunks), BF16),
        V((chunks, G, M, 2 * C // chunks), BF16), V((chunks, G, M, 2 * C // chunks), BF16),
        V((E, 1, M), F32), V((M, 2 * C), F32),
        V((T, M, C), BF16), V((T, M, C), BF16), V((T, 1, M), F32), V((E, 1, M), F32), V((1, 2 * M), F32),
        V((T * E, M, C), BF16), V((T, G, 2 * M, half), BF16),
        V((G, 2 * cap, D), BF16), V((slots, FH), BF16), V((G, 2 * cap, 2 * M), BF16),
        V((G, 2 * cap, M), BF16), V((G, 2 * cap, 128), F32), V((G, 2 * cap, 128), F32),
        V((2, G, 2 * cap, C), BF16), V((2, G, 2 * cap, C), BF16), V((2, G, 2 * cap, C), F32),
        V((G, 2 * cap, C), BF16), V((G, 2 * cap, C), BF16), V((E, cap, C), BF16), V((E, cap, C), BF16),
        V((2, M, C), F32),
        V((G, M, C), BF16), V((G, M, C), F32), V((G, M, C), BF16), V((G, M, C), BF16), V((G, M, C), BF16),
        V((G, M, C), BF16), V((M, C), BF16),
        DMA((8,)), DMA((12,)), DMA((1,)), DMA((1,)), DMA((chunks,)),
        DMA((1,)), DMA((G,)), DMA((1,)), DMA((1,)), DMA((1,)), DMA((1,)), DMA((1,)), DMA((chunks,)), DMA((chunks,)),
        DMA((1,)), DMA((1,)), DMA((1,)), DMA((1,)), DMA((1,)), DMA((1,)), DMA((1,)), DMA((1,)),
        DMA((1,)), DMA((4, G)), DMA((G,)), DMA((1,)), DMA((G,)), DMA((G,)),
        DMA((1,)), DMA((2,)), DMA((1,)), DMA((G,)), DMA((1,)), DMA((1,)),
        DMA((1,)), DMA((G,)), DMA((1,)), DMA((1,)), DMA((1,)), DMA((1,)),
    ]
    outs = pl.pallas_call(
        functools.partial(layer_kernel, E, T, cap),
        out_shape=(V((M, C), BF16), V((M, C), F32), V((conv_state.shape[1], M, C), BF16)),
        in_specs=[anyspace] * 21,
        out_specs=(vm, vm, vm),
        scratch_shapes=scratch,
        compiler_params=pltpu.CompilerParams(
            collective_id=0, has_side_effects=True, vmem_limit_bytes=60 * 1024 * 1024
        ),
    )(
        *small,
        proj_x, proj_y, dense_gate, dense_up, proj_out, expert_gate[0], expert_up[0], expert_down[0], dd,
    )
    new_hidden, new_lru, new_conv = pl.pallas_call(
        store_kernel,
        out_shape=tuple(jax.ShapeDtypeStruct(o.shape, o.dtype) for o in outs),
        in_specs=[vm] * 3,
        out_specs=(anyspace,) * 3,
        scratch_shapes=[DMA((3,))],
    )(*(pltpu.with_memory_space_constraint(o, pltpu.VMEM) for o in outs))
    return (new_hidden, new_lru, new_conv.transpose(1, 0, 2))


def solution(mesh):
    in_specs = (
        P("ep", None),
        P(),
        P("ep", "tp"),
        P("ep", "tp"),
        P(None, "tp"),
        P("tp", None, None),
        P("tp", None, None),
        P("tp"),
        P("tp", None),
        P("ep", None, "tp"),
        P("ep", "tp"),
        P(),
        P("ep", None),
        P("ep", None),
        P("ep", None, "tp"),
        P("ep", None, "tp"),
        P("ep", "tp", None),
        P("tp", "ep"),
        P("tp", "ep"),
        P("ep", "tp"),
        P("tp"),
    )
    out_specs = (P("ep", "tp"), P("ep", "tp"), P("ep", None, "tp"))
    return jax.shard_map(
        on_device, mesh=mesh, in_specs=in_specs, out_specs=out_specs, check_vma=False
    )
```
